512 devices in a mesh: grp: 2 (over y), sp: 32 (over z), tp: 8 (over x, core).
Axes of the slice: x: 4, y: 2, z: 32, core: 2. Of those that a mesh axis runs over, the one named last changes fastest.
The devices are a block of a 4x8x32 slice.
Arguments:
- queries: bfloat16 [32768, 1024], P(('grp', 'sp'), 'tp'), parts along dimension 0, may hold values from -120 to 120
- keys: bfloat16 [32768, 256], P(('grp', 'sp')), parts along dimension 0, may hold values from -6 to 6
- values: bfloat16 [32768, 256], P(('grp', 'sp')), parts along dimension 0, may hold values from -6 to 6
- sink: float32 [8], P('tp'), may hold values from 1 to 5
- resid: bfloat16 [32768, 2048], P(('grp', 'sp')), parts along dimension 0, may hold values from -100 to 100
- out_proj: bfloat16 [1024, 2048], P(None, 'tp'), may hold values from -1.5 to 1.5
- norm_gain: float32 [2048], replicated, may hold values from 0.1 to 1.9
- w_gate: bfloat16 [2048, 6144], P('sp', 'tp'), may hold values from -0.125 to 0.125
- w_up: bfloat16 [2048, 6144], P('sp', 'tp'), may hold values from -0.125 to 0.125
- conv_w: float32 [3, 6144], P(None, 'tp'), may hold values from -3 to 3
- conv_b: float32 [6144], P('tp'), may hold values from -3 to 3
- w_down: bfloat16 [6144, 2048], P('tp', 'sp'), may hold values from -0.3125 to 0.3125
Outputs:
- layer_out: bfloat16 [32768, 2048], P(('grp', 'sp'), 'tp'), parts along dimension 0
The draws below stay inside these ranges and needn't reach their ends.
There are 2 independent parts, one for each index of `grp`. The reference program is written for one: setup_inputs(seed, part) draws one part's arguments, and reference() takes and returns one part's arrays. A program takes and returns all parts, laid end to end along the dimension named above; an argument that names none is the same for every part. Nothing has to cross between parts.
All inputs are finite; a program needn't handle non-finite values.
Results may differ from the reference program's by a relative error of at most 0.015.
Values may be sent and summed in bfloat16 or wider, within the bound.
A program may use at most 64 MiB of HBM per device.

```python
import jax
import jax.numpy as jnp
from jax import lax

D = 2048
FF = 6144
H = 8
KVH = 2
HD = 128
WINDOW = 128
CONV = 3
TOK_DEV = 512
SEQ = 16384


def joint_qk(key):
    base = jax.random.fold_in(key, 11)
    key_q, key_k = jax.random.split(base)
    q_vals = jnp.clip(jax.random.normal(key_q, (SEQ, H, HD), jnp.float32), -6.0, 6.0)
    k_vals = jnp.clip(jax.random.normal(key_k, (SEQ, KVH, HD), jnp.float32), -6.0, 6.0)
    return (q_vals.reshape(SEQ, H * HD), k_vals.reshape(SEQ, KVH * HD))


def draw_queries(key, part):
    return joint_qk(key)[0].astype(jnp.bfloat16)


def draw_keys(key, part):
    return joint_qk(key)[1].astype(jnp.bfloat16)


def draw_resid(key, part):
    base = jax.random.fold_in(key, 23)
    key_n, key_r, key_c = jax.random.split(base, 3)
    trend = 0.5 + jnp.arange(D, dtype=jnp.float32) / D
    columns = jnp.exp(jax.random.uniform(key_c, (D,), jnp.float32, -0.7, 0.7)) * trend
    noise = jnp.clip(jax.random.normal(key_n, (SEQ, D), jnp.float32), -6.0, 6.0)
    rows = jnp.exp(jax.random.uniform(key_r, (SEQ, 1), jnp.float32, -0.69, 1.6))
    return jnp.clip(noise * rows * columns[None, :], -100.0, 100.0).astype(jnp.bfloat16)


def spiked(array, key, source, target, blocks, factor):
    def block_of(dim):
        return (jnp.arange(array.shape[dim]) // (array.shape[dim] // blocks)).reshape((-1,) + (1,) * (array.ndim - 1 - dim))

    first = jax.random.permutation(key, blocks)[block_of(target)]
    other_side = (block_of(target) + blocks // 2) % blocks
    return jnp.where((block_of(source) == first) | (block_of(source) == other_side), factor * array, array)


def steps_of(own_key, dims, cuts, least, high):
    loudness, own = 1.0, jax.random.fold_in(own_key, 6)
    for dim, parts in cuts:
        draws = jnp.exp(jax.random.uniform(jax.random.fold_in(own, dim), (parts,), jnp.float32, least / len(cuts), high / len(cuts)))
        loudness = loudness * jnp.repeat(draws, dims[dim] // parts).reshape([-1 if axis == dim else 1 for axis in range(len(dims))])
    return loudness


def gaussian(key, shape, scale, most, cuts=(), kind=jnp.bfloat16):
    drawn = scale * jax.random.normal(key, shape, jnp.float32)
    if cuts:
        drawn = drawn * steps_of(key, shape, cuts, -0.22, 0.18)
    return jnp.clip(drawn, -most, most).astype(kind)


def noise_with(own_key, extent, scale, reach, cuts, heavy, held_as=jnp.bfloat16):
    drawn = scale * jax.random.normal(own_key, extent, jnp.float32)
    if cuts:
        drawn = drawn * steps_of(own_key, extent, cuts, -0.22, 0.18)
    return jnp.clip(spiked(drawn, jax.random.fold_in(own_key, 3), *heavy), -reach, reach).astype(held_as)


def setup_inputs(seed: int = 0, part: int = 0) -> dict:
    key_list = jax.random.split(jax.random.key(seed), 13)
    own_keys = jax.random.split(jax.random.fold_in(key_list[12], part), 13)
    return {
        "queries": draw_queries(jax.random.fold_in(jax.random.fold_in(key_list[12], part), 71), part),
        "keys": draw_keys(jax.random.fold_in(jax.random.fold_in(key_list[12], part), 71), part),
        "values": gaussian(own_keys[2], (SEQ, KVH * HD), 1.0, 6.0, ((0, 32),)),
        "sink": jnp.clip(1.0 + 4.0 * jax.random.uniform(key_list[3], (H,), jnp.float32) ** steps_of(key_list[3], (H,), ((0, 8),), -0.2, 0.2), 1.0, 5.0),
        "resid": draw_resid(jax.random.fold_in(jax.random.fold_in(key_list[12], part), 71), part),
        "out_proj": gaussian(key_list[5], (H * HD, D), (H * HD // 64) ** -0.5, 1.5, ((1, 8),)),
        "norm_gain": jnp.clip(1.0 + 0.18 * jax.random.normal(key_list[6], (D,), jnp.float32), 0.1, 1.9),
        "w_gate": gaussian(key_list[7], (D, FF), D ** -0.5, 0.125, ((0, 32), (1, 8))),
        "w_up": gaussian(key_list[8], (D, FF), D ** -0.5, 0.125, ((0, 32), (1, 8))),
        "conv_w": gaussian(key_list[9], (CONV, FF), 0.6, 3.0, ((1, 8),), jnp.float32),
        "conv_b": gaussian(key_list[10], (FF,), 0.5, 3.0, ((0, 8),), jnp.float32),
        "w_down": noise_with(key_list[11], (FF, D), (FF // 4) ** -0.5, 0.3125, ((0, 8), (1, 32)), (0, 1, 32, 2.75)),
    }


def reference(queries, keys, values, sink, resid, out_proj, norm_gain, w_gate, w_up, conv_w, conv_b, w_down):
    group = H // KVH
    scale = HD ** (-0.5)
    span = TOK_DEV + 2 * WINDOW
    q_heads = queries.reshape(SEQ, H, HD)
    k_pad = jnp.pad(keys.reshape(SEQ, KVH, HD), ((WINDOW, WINDOW), (0, 0), (0, 0)))
    v_pad = jnp.pad(values.reshape(SEQ, KVH, HD), ((WINDOW, WINDOW), (0, 0), (0, 0)))
    sink_grid = sink.reshape(KVH, group)[:, :, None]

    def block(index):
        start = (index * TOK_DEV).astype(jnp.int32)
        q_block = lax.dynamic_slice_in_dim(q_heads, start, TOK_DEV, 0).astype(jnp.float32)
        q_block = q_block.reshape(TOK_DEV, KVH, group, HD)
        k_block = lax.dynamic_slice_in_dim(k_pad, start, span, 0).astype(jnp.float32)
        v_block = lax.dynamic_slice_in_dim(v_pad, start, span, 0).astype(jnp.float32)
        scores = jnp.einsum('qhgd,khd->hgqk', q_block, k_block) * scale
        q_pos = start + jnp.arange(TOK_DEV, dtype=jnp.int32)[:, None]
        k_pos = start - WINDOW + jnp.arange(span, dtype=jnp.int32)[None, :]
        valid = (jnp.abs(q_pos - k_pos) <= WINDOW) & (k_pos >= 0) & (k_pos < SEQ)
        scores = jnp.where(valid, scores, jnp.float32(-1e+30))
        top = jnp.maximum(lax.optimization_barrier(jnp.max(scores, axis=-1)), sink_grid)
        expo = jnp.exp(scores - top[..., None])
        total = lax.optimization_barrier(jnp.sum(expo, axis=-1)) + jnp.exp(sink_grid - top)
        weights = (expo / total[..., None]).astype(jnp.bfloat16)
        out = jnp.einsum('hgqk,khd->qhgd', weights.astype(jnp.float32), v_block)
        return out.astype(jnp.bfloat16).reshape(TOK_DEV, H * HD)
    mixed = lax.map(block, jnp.arange(SEQ // TOK_DEV, dtype=jnp.int32)).reshape(SEQ, H * HD)
    summed = resid.astype(jnp.float32) + jnp.dot(mixed, out_proj, preferred_element_type=jnp.float32)
    mean = lax.optimization_barrier(jnp.mean(summed, axis=-1, keepdims=True))
    msq = lax.optimization_barrier(jnp.mean(summed * summed, axis=-1, keepdims=True))
    normed = ((summed - mean) * lax.rsqrt(msq - mean * mean + 1e-05) * norm_gain).astype(jnp.bfloat16)
    gate_pre = jnp.dot(normed, w_gate, preferred_element_type=jnp.float32).astype(jnp.bfloat16)
    up_part = jnp.dot(normed, w_up, preferred_element_type=jnp.float32).astype(jnp.bfloat16)
    padded = jnp.pad(gate_pre.astype(jnp.float32), ((1, 1), (0, 0)))
    conv = conv_b
    for tap in range(CONV):
        conv = conv + padded[tap:tap + SEQ] * conv_w[tap]
    act = (jax.nn.silu(conv) * up_part.astype(jnp.float32)).astype(jnp.bfloat16)
    ffn = jnp.dot(act, w_down, preferred_element_type=jnp.float32)
    return (normed.astype(jnp.float32) + ffn).astype(jnp.bfloat16)
```

```python
import functools

import jax
import jax.numpy as jnp
from jax import lax
from jax.experimental import pallas as pl
from jax.experimental.pallas import tpu as pltpu
from jax.sharding import PartitionSpec as P

H = 8
KVH = 2
HD = 128
WINDOW = 128
CONV = 3
EDGE = 16
MESH = pl.DeviceIdType.MESH
F32 = jnp.float32
BF16 = jnp.bfloat16


def layer_kernel(
    span,
    ranks,
    q_hbm,
    k_hbm,
    v_hbm,
    sink_ref,
    res_hbm,
    op_hbm,
    gain_ref,
    wg_hbm,
    wu_hbm,
    cw_ref,
    cb_ref,
    wd_hbm,
    out_ref,
    q_buf,
    kv_buf,
    res_buf,
    op_buf,
    mix_buf,
    summed,
    stat,
    nx_buf,
    wide,
    tall,
    accs,
    act_buf,
    theirs_out,
    theirs_in,
    hop_out,
    hop_in,
    held,
    load_sem,
    kv_send,
    kv_recv,
    z_send,
    z_recv,
    y_send,
    y_recv,
    x_send,
    x_recv,
    edge_send,
    edge_recv,
    pair_send,
    pair_recv,
    hop_send,
    hop_recv,
):
    tokens, width = res_buf.shape
    depth, hidden = wg_hbm.shape
    cols = width // ranks
    half = span // 2
    pw = wide.shape[2]
    pd = tall.shape[2]
    chips = ranks // 2

    g = lax.axis_index("grp")
    s = lax.axis_index("sp")
    t = lax.axis_index("tp")
    right, left = lax.rem(s + 1, span), lax.rem(s + span - 1, span)
    parity = lax.rem(g, 2)
    pair_grp = g + 1 - 2 * parity
    own, other = 2 * parity, 2 - 2 * parity
    core = lax.rem(t, 2)
    chip = lax.div(t, 2)
    partner = t + 1 - 2 * core
    ahead = lax.rem(t + 2 - 4 * core + ranks, ranks)
    behind = lax.rem(t - 2 + 4 * core + ranks, ranks)
    across = lax.rem(t + ranks // 2, ranks)
    kv_col = pl.multiple_of(lax.div(t * KVH, ranks) * HD, HD)

    def rows(j):
        return pl.ds(pl.multiple_of(j * depth, depth), depth)

    own_rows = rows(s)
    cut = pw - (hidden - pw)
    loads = [
        (wg_hbm.at[:, pl.ds(0, pw)], wide.at[0, own_rows, :]),
        (wg_hbm.at[:, pl.ds(pw, hidden - pw)], wide.at[1, own_rows, pl.ds(0, hidden - pw)]),
        (wu_hbm.at[:, pl.ds(0, cut)], wide.at[1, own_rows, pl.ds(hidden - pw, cut)]),
        (wu_hbm.at[:, pl.ds(cut, pw)], wide.at[2, own_rows, :]),
        (wd_hbm.at[:, pl.ds(0, pd)], tall.at[0, own_rows, :]),
        (wd_hbm.at[:, pl.ds(pd, pd)], tall.at[1, own_rows, :]),
        (wd_hbm.at[:, pl.ds(2 * pd, pd)], tall.at[2, own_rows, :]),
        (k_hbm.at[:, pl.ds(kv_col, HD)], kv_buf.at[0, pl.ds(WINDOW, tokens), :]),
        (v_hbm.at[:, pl.ds(kv_col, HD)], kv_buf.at[1, pl.ds(WINDOW, tokens), :]),
        (q_hbm, q_buf),
        (op_hbm, op_buf.at[t]),
        (res_hbm, res_buf),
    ]
    loads = [pltpu.make_async_copy(a, b, load_sem.at[i]) for i, (a, b) in enumerate(loads)]

    barrier = pltpu.get_barrier_semaphore()
    greeted = ({"sp": right}, {"sp": left}, {"grp": pair_grp}, {"tp": ahead}, {"tp": behind}, {"tp": partner})
    for who in greeted:
        pl.semaphore_signal(barrier, inc=1, device_id=who, device_id_type=MESH)
    for copy in loads:
        copy.start()

    def remote(src, dst, send, recv, who):
        return pltpu.make_async_remote_copy(
            src_ref=src, dst_ref=dst, send_sem=send, recv_sem=recv, device_id=who, device_id_type=MESH
        )

    def part(kind, index, j):
        return (wide if kind == 0 else tall).at[index, rows(j), :]

    def z_copy(kind, ab, j, way):
        ref = part(kind, own if ab else 1, j)
        row = 2 * kind + ab
        return remote(ref, ref, z_send.at[way, row], z_recv.at[row, j], {"sp": left if way else right})

    def y_copy(kind, j):
        ref = part(kind, own, j)
        return remote(ref, ref, y_send.at[kind], y_recv.at[kind, j], {"grp": pair_grp})

    def y_arrived(kind, j):
        ref = part(kind, other, j)
        remote(ref, ref, y_send.at[kind], y_recv.at[kind, j], {"grp": pair_grp}).wait_recv()

    def block(kind, b):
        if kind == 0:
            return op_buf.at[b]
        return mix_buf.at[:, pl.ds(pl.multiple_of(b * HD, HD), HD)]

    def x_copy(kind, b, slot, who):
        ref = block(kind, b)
        return remote(ref, ref, x_send.at[kind, slot], x_recv.at[kind, b], {"tp": who})

    def x_open(kind):
        x_copy(kind, t, 0, ahead).start()
        x_copy(kind, t, 1, behind).start()
        x_copy(kind, t, 2, partner).start()

    def x_pass(kind):
        x_copy(kind, behind, 3, ahead).wait_recv()
        x_copy(kind, behind, 3, ahead).start()
        x_copy(kind, behind, 4, partner).start()
        x_copy(kind, ahead, 5, partner).wait_recv()
        x_copy(kind, ahead, 5, partner).start()

    def x_last(kind):
        x_copy(kind, across, 6, partner).wait_recv()
        x_copy(kind, across, 6, partner).start()

    def x_close(kind):
        for step in range(chips):
            b = lax.rem(partner + 2 * step, ranks)
            x_copy(kind, b, 0, partner).wait_recv()

    def kv_copy(way):
        if way == 0:
            src, dst = kv_buf.at[:, pl.ds(tokens, WINDOW), :], kv_buf.at[:, pl.ds(0, WINDOW), :]
        else:
            src, dst = kv_buf.at[:, pl.ds(WINDOW, WINDOW), :], kv_buf.at[:, pl.ds(WINDOW + tokens, WINDOW), :]
        return remote(src, dst, kv_send.at[way], kv_recv.at[way], {"sp": left if way else right})

    def edge_copy(way):
        if way == 0:
            src, dst = nx_buf.at[pl.ds(tokens, EDGE), :], nx_buf.at[pl.ds(0, EDGE), :]
        else:
            src, dst = nx_buf.at[pl.ds(EDGE, EDGE), :], nx_buf.at[pl.ds(EDGE + tokens, EDGE), :]
        return remote(src, dst, edge_send.at[way], edge_recv.at[way], {"sp": left if way else right})

    def attend(i):
        lo = i * WINDOW
        keys = kv_buf[0, lo : lo + 3 * WINDOW, :]
        vals = kv_buf[1, lo : lo + 3 * WINDOW, :]
        scores = lax.dot_general(
            q_buf[lo : lo + WINDOW, :], keys, (((1,), (1,)), ((), ())), preferred_element_type=F32
        ) * (HD ** (-0.5))
        row = lax.broadcasted_iota(jnp.int32, scores.shape, 0)
        col = lax.broadcasted_iota(jnp.int32, scores.shape, 1)
        pos = s * tokens + (lo - WINDOW) + col
        gap = col - row
        seen = (gap >= 0) & (gap <= 2 * WINDOW) & (pos >= 0) & (pos < span * tokens)
        scores = jnp.where(seen, scores, F32(-1e30))
        sink = sink_ref[0]
        top = jnp.maximum(jnp.max(scores, axis=-1, keepdims=True), sink)
        expo = jnp.exp(scores - top)
        total = jnp.sum(expo, axis=-1, keepdims=True) + jnp.exp(sink - top)
        weights = (expo / total).astype(BF16)
        mixed = jnp.dot(weights, vals, preferred_element_type=F32).astype(BF16)
        mix_buf[lo : lo + WINDOW, pl.ds(pl.multiple_of(t * HD, HD), HD)] = mixed

    def project(o):
        at = slice(o * cols, (o + 1) * cols)
        block_sum = res_buf[:, at].astype(F32) + jnp.dot(mix_buf[...], op_buf[o], preferred_element_type=F32)
        summed[:, at] = block_sum
        first, second = block_sum[:, : cols // 2], block_sum[:, cols // 2 :]
        lone = first + second
        squares = first * first + second * second
        if o == 0:
            stat[0] = lone
            stat[1] = squares
        else:
            stat[0] += lone
            stat[1] += squares

    def normalize(lo, hi):
        @pl.loop(lo // EDGE, hi // EDGE)
        def _(i):
            at = pl.ds(pl.multiple_of(i * EDGE, EDGE), EDGE)
            mean = jnp.sum(stat[0, at, :], axis=-1, keepdims=True) / width
            msq = jnp.sum(stat[1, at, :], axis=-1, keepdims=True) / width
            scale = lax.rsqrt(msq - mean * mean + 1e-05)
            normed = (summed[at, :] - mean) * scale * gain_ref[...]
            nx_buf[pl.ds(pl.multiple_of(i * EDGE + EDGE, EDGE), EDGE), :] = normed.astype(BF16)

    quads = span * depth // cols
    mine = lax.div(s * depth, cols)

    def gates(shift, first=False):
        quad = lax.rem(mine + shift + quads, quads)
        for i in range(cols // depth):
            j = quad * (cols // depth) + i

            @pl.when(j != s)
            def _():
                y_arrived(0, j)

        at = pl.ds(pl.multiple_of(quad * cols, cols), cols)
        x = nx_buf[:, at]
        for p in range(3):
            y = jnp.dot(x, wide[p, at, :], preferred_element_type=F32)
            if first:
                accs[p] = y
            else:
                accs[p] += y

    def edge_zero(where):
        for p in range(2):
            accs[p, where : where + EDGE, :] = jnp.zeros((EDGE, pw), F32)

    def activate():
        for h in range(3):
            gp, gc = divmod(h * pd, pw)
            up, uc = divmod(hidden + h * pd, pw)
            for r in range(0, tokens, WINDOW):
                conv = cb_ref[h * pd : (h + 1) * pd].reshape(1, pd)
                for tap in range(CONV):
                    lo = EDGE - CONV // 2 + tap + r
                    gate = accs[gp, lo : lo + WINDOW, gc : gc + pd].astype(BF16).astype(F32)
                    conv = conv + gate * cw_ref[tap : tap + 1, h * pd : (h + 1) * pd]
                ups = accs[up, EDGE + r : EDGE + r + WINDOW, uc : uc + pd].astype(BF16).astype(F32)
                act = conv / (1.0 + jnp.exp(-conv)) * ups
                act_buf[r : r + WINDOW, h * pd : (h + 1) * pd] = act.astype(BF16)

    def partial(o):
        at = pl.ds(pl.multiple_of(o * cols, cols), cols)
        total = None
        for p in range(3):
            term = lax.dot_general(
                act_buf[:, p * pd : (p + 1) * pd],
                tall[p, at, :],
                (((1,), (1,)), ((), ())),
                preferred_element_type=F32,
            )
            total = term if total is None else total + term
        return total

    def pair_copy(owner):
        return remote(
            theirs_out.at[owner], theirs_in.at[owner], pair_send.at[owner], pair_recv.at[owner], {"tp": partner}
        )

    def hop_copy(i):
        return remote(hop_out.at[i], hop_in.at[i], hop_send.at[i], hop_recv.at[i], {"tp": behind if i == 1 else ahead})

    def give(owner):
        theirs_out[owner] = partial(2 * owner + 1 - core).astype(BF16)

    def joined(owner):
        kept = partial(2 * owner + core)
        pair_copy(owner).wait_recv()
        return kept + theirs_in[owner].astype(F32)

    for i in range(9):
        loads[i].wait()
    pl.semaphore_wait(barrier, len(greeted))
    for way in range(2):
        kv_copy(way).start()
    for kind in range(2):
        for ab in range(2):
            for way in range(2):
                z_copy(kind, ab, s, way).start()
    loads[10].wait()
    x_open(0)
    loads[9].wait()

    def unit_attend(blocks, last):
        if not last:
            for way in range(2):
                kv_copy(way).wait_recv()
        for i in blocks:
            attend(i)
        if last:
            x_open(1)

    def unit_last():
        x_last(0)
        x_last(1)

    def unit_project(blocks):
        if blocks[0] == 0:
            x_close(0)
            x_close(1)
            loads[11].wait()
        for o in blocks:
            project(o)

    def unit_normalize(lo, hi):
        normalize(lo, hi)
        if hi == tokens:
            for way in range(2):
                edge_copy(way).start()

    def unit_gates(shifts, first=False):
        if first:
            for way in range(2):
                edge_copy(way).wait_recv()
        for i, shift in enumerate(shifts):
            gates(shift, first and i == 0)

    blocks = tokens // WINDOW
    units = {
        (1, 0): lambda: unit_attend(range(blocks // 2), False),
        (1, 1): lambda: unit_attend(range(blocks // 2, blocks), True),
        (3, 1): lambda: x_pass(0),
        (4, 0): lambda: x_pass(1),
        (5, 1): unit_last,
        (6, 0): lambda: unit_project([0, 1]),
        (6, 1): lambda: unit_project([2, 3]),
        (7, 0): lambda: unit_project([4, 5]),
        (7, 1): lambda: unit_project([6, 7]),
        (8, 0): lambda: unit_normalize(0, tokens // 2),
        (8, 1): lambda: unit_normalize(tokens // 2, tokens),
        (9, 1): lambda: unit_gates([0], True),
        (10, 0): lambda: unit_gates([1]),
        (10, 1): lambda: unit_gates([-1]),
        (12, 0): lambda: unit_gates([2]),
        (12, 1): lambda: unit_gates([-2]),
    }

    @pl.loop(1, half)
    def _(k):
        back = lax.rem(s - k + span, span)
        front = lax.rem(s + k, span)
        for kind in range(2):
            for ab in range(2):
                for way, j in ((0, back), (1, front)):
                    z_copy(kind, ab, j, way).wait_recv()
                    if ab == way:
                        z_copy(kind, ab, j, way).start()
                    else:

                        @pl.when(k < half - 1)
                        def _():
                            z_copy(kind, ab, j, way).start()

                    if ab == 1:
                        y_copy(kind, j).start()
            for (step, slot), unit in units.items():
                if slot == kind:
                    pl.when(k == step)(unit)

    far = lax.rem(s + half, span)
    for kind in range(2):
        z_copy(kind, 0, far, 0).wait_recv()
        z_copy(kind, 1, far, 1).wait_recv()
        y_copy(kind, far).start()

    gates(3)
    gates(-3)
    gates(4)

    @pl.when(s == 0)
    def _():
        edge_zero(0)

    @pl.when(s == span - 1)
    def _():
        edge_zero(EDGE + tokens)

    activate()

    @pl.loop(1, span)
    def _(k):
        y_arrived(1, lax.rem(s + k, span))

    chip_across = lax.div(across, 2)
    chip_ahead = lax.div(ahead, 2)
    chip_behind = lax.div(behind, 2)
    give(chip_across)
    give(chip_behind)
    pair_copy(chip_across).start()
    give(chip_ahead)
    pair_copy(chip_behind).start()
    pair_copy(chip_ahead).start()
    hop_out[0] = joined(chip_across).astype(BF16)
    hop_copy(0).start()
    hop_out[1] = joined(chip_behind).astype(BF16)
    give(chip)
    hop_copy(1).start()
    pair_copy(chip).start()
    held[0] = joined(chip_ahead)
    own_cols = pl.ds(pl.multiple_of(t * cols, cols), cols)
    held[1] = joined(chip) + nx_buf[EDGE : EDGE + tokens, own_cols].astype(F32)
    hop_copy(0).wait_recv()
    hop_out[2] = (held[0] + hop_in[0].astype(F32)).astype(BF16)
    hop_copy(2).start()
    hop_copy(1).wait_recv()
    held[1] += hop_in[1].astype(F32)
    hop_copy(2).wait_recv()
    out_ref[...] = (held[1] + hop_in[2].astype(F32)).astype(BF16)

    for way in range(2):
        kv_copy(way).wait_send()
        edge_copy(way).wait_send()
        for kind in range(2):
            for ab in range(2):
                n = half if ab == way else half - 1
                ref = (wide if kind == 0 else tall).at[0, pl.ds(0, n * depth), :]
                row = 2 * kind + ab
                remote(ref, ref, z_send.at[way, row], z_recv.at[row, 0], {"sp": right}).wait_send()
    for kind in range(2):
        ref = (wide if kind == 0 else tall).at[0, pl.ds(0, (span - 1) * depth), :]
        remote(ref, ref, y_send.at[kind], y_recv.at[kind, 0], {"grp": pair_grp}).wait_send()
        for slot in range(7):
            x_copy(kind, t, slot, partner).wait_send()
    for owner in range(chips):
        pair_copy(owner).wait_send()
    for i in range(3):
        hop_copy(i).wait_send()


def solution(mesh):
    span, ranks = mesh.shape["sp"], mesh.shape["tp"]

    def shards(q, k, v, sink, resid, out_proj, gain, w_gate, w_up, conv_w, conv_b, w_down):
        tokens, width = resid.shape
        depth, hidden = w_gate.shape
        cols = width // ranks
        chips = ranks // 2
        pw, pd = 2 * hidden // 3, hidden // 3
        whole = pl.BlockSpec(memory_space=pltpu.VMEM)
        there = pl.BlockSpec(memory_space=pl.ANY)
        scalar = pl.BlockSpec(memory_space=pltpu.SMEM)
        dma = pltpu.SemaphoreType.DMA
        return pl.pallas_call(
            functools.partial(layer_kernel, span, ranks),
            out_shape=jax.ShapeDtypeStruct((tokens, cols), BF16),
            in_specs=[there, there, there, scalar, there, there, whole, there, there, whole, whole, there],
            out_specs=whole,
            scratch_shapes=[
                pltpu.VMEM((tokens, HD), BF16),
                pltpu.VMEM((2, tokens + 2 * WINDOW, HD), BF16),
                pltpu.VMEM((tokens, width), BF16),
                pltpu.VMEM((ranks, out_proj.shape[0], cols), BF16),
                pltpu.VMEM((tokens, ranks * HD), BF16),
                pltpu.VMEM((tokens, width), F32),
                pltpu.VMEM((2, tokens, cols // 2), F32),
                pltpu.VMEM((tokens + 2 * EDGE, width), BF16),
                pltpu.VMEM((3, span * depth, pw), BF16),
                pltpu.VMEM((3, span * depth, pd), BF16),
                pltpu.VMEM((3, tokens + 2 * EDGE, pw), F32),
                pltpu.VMEM((tokens, hidden), BF16),
                pltpu.VMEM((chips, tokens, cols), BF16),
                pltpu.VMEM((chips, tokens, cols), BF16),
                pltpu.VMEM((3, tokens, cols), BF16),
                pltpu.VMEM((3, tokens, cols), BF16),
                pltpu.VMEM((2, tokens, cols), F32),
                dma((12,)),
                dma((2,)),
                dma((2,)),
                dma((2, 4)),
                dma((4, span)),
                dma((2,)),
                dma((2, span)),
                dma((2, 7)),
                dma((2, ranks)),
                dma((2,)),
                dma((2,)),
                dma((chips,)),
                dma((chips,)),
                dma((3,)),
                dma((3,)),
            ],
            compiler_params=pltpu.CompilerParams(
                collective_id=0, has_side_effects=True, vmem_limit_bytes=60 * 1024 * 1024
            ),
        )(
            q, k, v, sink, resid, out_proj, gain.reshape(1, width), w_gate, w_up,
            conv_w, conv_b, w_down.T,
        )

    return jax.shard_map(
        shards,
        mesh=mesh,
        in_specs=(
            P(("grp", "sp"), "tp"),
            P(("grp", "sp"), None),
            P(("grp", "sp"), None),
            P("tp"),
            P(("grp", "sp"), None),
            P(None, "tp"),
            P(),
            P("sp", "tp"),
            P("sp", "tp"),
            P(None, "tp"),
            P("tp"),
            P("tp", "sp"),
        ),
        out_specs=P(("grp", "sp"), "tp"),
        check_vma=False,
    )
```

```python
import functools

import jax
import jax.numpy as jnp
from jax import lax
from jax.experimental import pallas as pl
from jax.experimental.pallas import tpu as pltpu
from jax.sharding import PartitionSpec as P

H = 8
KVH = 2
HD = 128
WINDOW = 128
CONV = 3
EDGE = 16
MESH = pl.DeviceIdType.MESH
F32 = jnp.float32
BF16 = jnp.bfloat16


def layer_kernel(
    span,
    ranks,
    q_hbm,
    k_hbm,
    v_hbm,
    sink_ref,
    res_hbm,
    op_hbm,
    gain_hbm,
    wg_hbm,
    wu_hbm,
    cw_hbm,
    cb_hbm,
    wd_hbm,
    out_ref,
    gain_ref,
    cw_ref,
    cb_ref,
    q_buf,
    kv_buf,
    res_buf,
    op_buf,
    mix_buf,
    summed,
    stat,
    nx_buf,
    wide,
    tall,
    accs,
    act_buf,
    theirs_out,
    theirs_in,
    hop_out,
    hop_in,
    held,
    out_buf,
    out_sem,
    load_sem,
    kv_send,
    kv_recv,
    z_send,
    z_recv,
    y_send,
    y_recv,
    x_send,
    x_recv,
    edge_send,
    edge_recv,
    pair_send,
    pair_recv,
    hop_send,
    hop_recv,
):
    tokens, width = res_buf.shape
    depth, hidden = wg_hbm.shape
    cols = width // ranks
    half = span // 2
    pw = wide.shape[2]
    pd = tall.shape[2]
    chips = ranks // 2

    g = lax.axis_index("grp")
    s = lax.axis_index("sp")
    t = lax.axis_index("tp")
    right, left = lax.rem(s + 1, span), lax.rem(s + span - 1, span)
    parity = lax.rem(g, 2)
    pair_grp = g + 1 - 2 * parity
    own, other = 2 * parity, 2 - 2 * parity
    core = lax.rem(t, 2)
    chip = lax.div(t, 2)
    partner = t + 1 - 2 * core
    ahead = lax.rem(t + 2 - 4 * core + ranks, ranks)
    behind = lax.rem(t - 2 + 4 * core + ranks, ranks)
    across = lax.rem(t + ranks // 2, ranks)
    kv_col = pl.multiple_of(lax.div(t * KVH, ranks) * HD, HD)

    def scoped(name, fn):
        def run():
            with jax.named_scope(name):
                fn()

        return run

    def rows(j):
        return pl.ds(pl.multiple_of(j * depth, depth), depth)

    own_rows = rows(s)
    cut = pw - (hidden - pw)
    loads = [
        (wg_hbm.at[:, pl.ds(0, pw)], wide.at[0, own_rows, :]),
        (wg_hbm.at[:, pl.ds(pw, hidden - pw)], wide.at[1, own_rows, pl.ds(0, hidden - pw)]),
        (wu_hbm.at[:, pl.ds(0, cut)], wide.at[1, own_rows, pl.ds(hidden - pw, cut)]),
        (wu_hbm.at[:, pl.ds(cut, pw)], wide.at[2, own_rows, :]),
        (wd_hbm.at[:, pl.ds(0, pd)], tall.at[0, own_rows, :]),
        (wd_hbm.at[:, pl.ds(pd, pd)], tall.at[1, own_rows, :]),
        (wd_hbm.at[:, pl.ds(2 * pd, pd)], tall.at[2, own_rows, :]),
        (k_hbm.at[:, pl.ds(kv_col, HD)], kv_buf.at[0, pl.ds(WINDOW, tokens), :]),
        (v_hbm.at[:, pl.ds(kv_col, HD)], kv_buf.at[1, pl.ds(WINDOW, tokens), :]),
        (q_hbm, q_buf),
        (op_hbm, op_buf.at[t]),
        (res_hbm, res_buf),
        (gain_hbm, gain_ref),
        (cw_hbm, cw_ref),
        (cb_hbm, cb_ref),
    ]
    loads = [pltpu.make_async_copy(a, b, load_sem.at[i]) for i, (a, b) in enumerate(loads)]

    barrier = pltpu.get_barrier_semaphore()
    greeted = ({"sp": right}, {"sp": left}, {"grp": pair_grp}, {"tp": ahead}, {"tp": behind}, {"tp": partner})
    for who in greeted:
        pl.semaphore_signal(barrier, inc=1, device_id=who, device_id_type=MESH)
    for copy in loads:
        copy.start()

    def remote(src, dst, send, recv, who):
        return pltpu.make_async_remote_copy(
            src_ref=src, dst_ref=dst, send_sem=send, recv_sem=recv, device_id=who, device_id_type=MESH
        )

    def part(kind, index, j):
        return (wide if kind == 0 else tall).at[index, rows(j), :]

    def z_copy(kind, ab, j, way):
        ref = part(kind, own if ab else 1, j)
        row = 2 * kind + ab
        return remote(ref, ref, z_send.at[way, row], z_recv.at[row, j], {"sp": left if way else right})

    def y_copy(kind, j):
        ref = part(kind, own, j)
        return remote(ref, ref, y_send.at[kind], y_recv.at[kind, j], {"grp": pair_grp})

    def y_arrived(kind, j):
        ref = part(kind, other, j)
        remote(ref, ref, y_send.at[kind], y_recv.at[kind, j], {"grp": pair_grp}).wait_recv()

    def block(kind, b):
        if kind == 0:
            return op_buf.at[b]
        return mix_buf.at[:, pl.ds(pl.multiple_of(b * HD, HD), HD)]

    def x_copy(kind, b, slot, who):
        ref = block(kind, b)
        return remote(ref, ref, x_send.at[kind, slot], x_recv.at[kind, b], {"tp": who})

    def x_open(kind):
        x_copy(kind, t, 0, ahead).start()
        x_copy(kind, t, 1, behind).start()
        x_copy(kind, t, 2, partner).start()

    def x_pass(kind):
        x_copy(kind, behind, 3, ahead).wait_recv()
        x_copy(kind, behind, 3, ahead).start()
        x_copy(kind, behind, 4, partner).start()
        x_copy(kind, ahead, 5, partner).wait_recv()
        x_copy(kind, ahead, 5, partner).start()

    def x_last(kind):
        x_copy(kind, across, 6, partner).wait_recv()
        x_copy(kind, across, 6, partner).start()

    def x_close(kind):
        for step in range(chips):
            b = lax.rem(partner + 2 * step, ranks)
            x_copy(kind, b, 0, partner).wait_recv()

    def kv_copy(way):
        if way == 0:
            src, dst = kv_buf.at[:, pl.ds(tokens, WINDOW), :], kv_buf.at[:, pl.ds(0, WINDOW), :]
        else:
            src, dst = kv_buf.at[:, pl.ds(WINDOW, WINDOW), :], kv_buf.at[:, pl.ds(WINDOW + tokens, WINDOW), :]
        return remote(src, dst, kv_send.at[way], kv_recv.at[way], {"sp": left if way else right})

    def edge_copy(way):
        if way == 0:
            src, dst = nx_buf.at[pl.ds(tokens, EDGE), :], nx_buf.at[pl.ds(0, EDGE), :]
        else:
            src, dst = nx_buf.at[pl.ds(EDGE, EDGE), :], nx_buf.at[pl.ds(EDGE + tokens, EDGE), :]
        return remote(src, dst, edge_send.at[way], edge_recv.at[way], {"sp": left if way else right})

    def attend(i):
        lo = i * WINDOW
        keys = kv_buf[0, lo : lo + 3 * WINDOW, :]
        vals = kv_buf[1, lo : lo + 3 * WINDOW, :]
        scores = lax.dot_general(
            q_buf[lo : lo + WINDOW, :], keys, (((1,), (1,)), ((), ())), preferred_element_type=F32
        ) * (HD ** (-0.5))
        row = lax.broadcasted_iota(jnp.int32, scores.shape, 0)
        col = lax.broadcasted_iota(jnp.int32, scores.shape, 1)
        pos = s * tokens + (lo - WINDOW) + col
        gap = col - row
        seen = (gap >= 0) & (gap <= 2 * WINDOW) & (pos >= 0) & (pos < span * tokens)
        scores = jnp.where(seen, scores, F32(-1e30))
        sink = sink_ref[0]
        top = jnp.maximum(jnp.max(scores, axis=-1, keepdims=True), sink)
        expo = jnp.exp(scores - top)
        total = jnp.sum(expo, axis=-1, keepdims=True) + jnp.exp(sink - top)
        weights = (expo / total).astype(BF16)
        mixed = jnp.dot(weights, vals, preferred_element_type=F32).astype(BF16)
        mix_buf[lo : lo + WINDOW, pl.ds(pl.multiple_of(t * HD, HD), HD)] = mixed

    def project(o, opens):
        at = pl.ds(pl.multiple_of(o * cols, cols), cols)
        block_sum = res_buf[:, at].astype(F32) + jnp.dot(mix_buf[...], op_buf[o], preferred_element_type=F32)
        summed[:, at] = block_sum
        first, second = block_sum[:, : cols // 2], block_sum[:, cols // 2 :]
        lone = first + second
        squares = first * first + second * second
        if opens:
            stat[0] = lone
            stat[1] = squares
        else:
            stat[0] += lone
            stat[1] += squares

    def normalize(lo, hi):
        @pl.loop(lo // EDGE, hi // EDGE)
        def _(i):
            at = pl.ds(pl.multiple_of(i * EDGE, EDGE), EDGE)
            mean = jnp.sum(stat[0, at, :], axis=-1, keepdims=True) / width
            msq = jnp.sum(stat[1, at, :], axis=-1, keepdims=True) / width
            scale = lax.rsqrt(msq - mean * mean + 1e-05)
            normed = (summed[at, :] - mean) * scale * gain_ref[...]
            nx_buf[pl.ds(pl.multiple_of(i * EDGE + EDGE, EDGE), EDGE), :] = normed.astype(BF16)

    mid = tokens // 2
    lots = [slice(0, mid), slice(mid, tokens)]
    quads = span * depth // cols
    mine = lax.div(s * depth, cols)

    def gates(shift, first=False):
        quad = lax.rem(mine + shift + quads, quads)
        for i in range(cols // depth):
            j = quad * (cols // depth) + i

            @pl.when(j != s)
            def _():
                y_arrived(0, j)

        at = pl.ds(pl.multiple_of(quad * cols, cols), cols)
        x = nx_buf[:, at]
        for p in range(3):
            y = jnp.dot(x, wide[p, at, :], preferred_element_type=F32)
            if first:
                accs[p] = y
            else:
                accs[p] += y

    def edge_zero(where):
        for p in range(2):
            accs[p, where : where + EDGE, :] = jnp.zeros((EDGE, pw), F32)

    def activate(half_of):
        for h in range(3):
            gp, gc = divmod(h * pd, pw)
            up, uc = divmod(hidden + h * pd, pw)
            for r in range(half_of * mid, (half_of + 1) * mid, WINDOW):
                conv = cb_ref[h * pd : (h + 1) * pd].reshape(1, pd)
                for tap in range(CONV):
                    lo = EDGE - CONV // 2 + tap + r
                    gate = accs[gp, lo : lo + WINDOW, gc : gc + pd].astype(BF16).astype(F32)
                    conv = conv + gate * cw_ref[tap : tap + 1, h * pd : (h + 1) * pd]
                ups = accs[up, EDGE + r : EDGE + r + WINDOW, uc : uc + pd].astype(BF16).astype(F32)
                act = conv / (1.0 + jnp.exp(-conv)) * ups
                act_buf[r : r + WINDOW, h * pd : (h + 1) * pd] = act.astype(BF16)

    def partial(o, lot):
        at = pl.ds(pl.multiple_of(o * cols, cols), cols)
        total = None
        for p in range(3):
            term = lax.dot_general(
                act_buf[lot, p * pd : (p + 1) * pd],
                tall[p, at, :],
                (((1,), (1,)), ((), ())),
                preferred_element_type=F32,
            )
            total = term if total is None else total + term
        return total

    def pair_copy(owner, h):
        src, dst = theirs_out.at[owner, lots[h]], theirs_in.at[owner, lots[h]]
        return remote(src, dst, pair_send.at[owner, h], pair_recv.at[owner, h], {"tp": partner})

    def hop_copy(i, h):
        src, dst = hop_out.at[i, lots[h]], hop_in.at[i, lots[h]]
        return remote(src, dst, hop_send.at[i, h], hop_recv.at[i, h], {"tp": behind if i == 1 else ahead})

    def out_copy(h):
        return pltpu.make_async_copy(out_buf.at[lots[h], :], out_ref.at[lots[h], :], out_sem.at[h])

    def give(owner, h):
        theirs_out[owner, lots[h]] = partial(2 * owner + 1 - core, lots[h]).astype(BF16)
        pair_copy(owner, h).start()

    def joined(owner, h):
        kept = partial(2 * owner + core, lots[h])
        pair_copy(owner, h).wait_recv()
        return kept + theirs_in[owner, lots[h]].astype(F32)

    def hop(i, owner, h):
        hop_out[i, lots[h]] = joined(owner, h).astype(BF16)
        hop_copy(i, h).start()

    with jax.named_scope('load'):
        for i in range(9):
            loads[i].wait()
    with jax.named_scope('bar'):
        pl.semaphore_wait(barrier, len(greeted))
    for way in range(2):
        kv_copy(way).start()
    for kind in range(2):
        for turn in range(2):
            for way in range(2):
                z_copy(kind, turn if way == 0 else 1 - turn, s, way).start()
    loads[10].wait()
    x_open(0)
    loads[9].wait()

    def unit_attend(blocks, last):
        if not last:
            for way in range(2):
                kv_copy(way).wait_recv()
        for i in blocks:
            attend(i)
        if last:
            x_open(1)

    def mirror(b):
        return b + 1 - 2 * lax.rem(b, 2)

    def unit_project(stage):
        if stage == 0:
            x_close(1)
            for i in range(11, 15):
                loads[i].wait()
            project(t, True)
            project(ahead, False)
        if stage == 1:
            x_last(0)
            x_copy(0, partner, 0, partner).wait_recv()
            project(behind, False)
            project(partner, False)
        if stage == 2:
            for b in (mirror(ahead), mirror(behind)):
                x_copy(0, b, 0, partner).wait_recv()
                project(b, False)
        if stage == 3:
            x_copy(0, mirror(across), 0, partner).wait_recv()
            project(across, False)
            project(mirror(across), False)

    quarter = tokens // 4

    def unit_normalize(i, send=False):
        normalize(i * quarter, (i + 1) * quarter)
        if send:
            for way in range(2):
                edge_copy(way).start()

    def unit_gates(shifts, first=False):
        if first:
            for way in range(2):
                edge_copy(way).wait_recv()
        for i, shift in enumerate(shifts):
            gates(shift, first and i == 0)

    blocks = tokens // WINDOW
    units = {
        (1, 0): lambda: unit_attend(range(blocks // 2), False),
        (1, 1): lambda: unit_attend(range(blocks // 2, blocks), True),
        (3, 0): lambda: x_pass(0),
        (3, 1): lambda: x_pass(1),
        (5, 0): lambda: x_last(1),
        (6, 0): lambda: unit_project(0),
        (6, 1): lambda: unit_project(1),
        (7, 0): lambda: unit_project(2),
        (7, 1): lambda: unit_project(3),
        (8, 0): lambda: unit_normalize(0),
        (8, 1): lambda: unit_normalize(3, True),
        (9, 0): lambda: unit_normalize(1),
        (9, 1): lambda: unit_normalize(2),
        (10, 0): lambda: unit_gates([0], True),
        (10, 1): lambda: unit_gates([1]),
        (11, 0): lambda: unit_gates([-1]),
        (12, 1): lambda: unit_gates([2]),
        (13, 0): lambda: unit_gates([-2]),
    }

    @pl.loop(1, half)
    def _(k):
        back = lax.rem(s - k + span, span)
        front = lax.rem(s + k, span)
        for kind in range(2):
            with jax.named_scope(f'hop{kind}'):
                for turn in range(2):
                    for way, j in ((0, back), (1, front)):
                        ab = turn if way == 0 else 1 - turn
                        z_copy(kind, ab, j, way).wait_recv()
                        if ab == way:
                            z_copy(kind, ab, j, way).start()
                        else:

                            @pl.when(k < half - 1)
                            def _():
                                z_copy(kind, ab, j, way).start()

                        if ab == 1:
                            y_copy(kind, j).start()
            for (step, slot), unit in units.items():
                if slot == kind:
                    pl.when(k == step)(scoped(f'u{step}_{slot}', unit))

    far = lax.rem(s + half, span)
    for kind in range(2):
        with jax.named_scope(f'far{kind}'):
            z_copy(kind, 1, far, 1).wait_recv()
            y_copy(kind, far).start()
            z_copy(kind, 0, far, 0).wait_recv()

    with jax.named_scope('gate3'):
        gates(3)
    with jax.named_scope('gate3'):
        gates(-3)
    with jax.named_scope('gate4'):
        gates(4)

    @pl.when(s == 0)
    def _():
        edge_zero(0)

    @pl.when(s == span - 1)
    def _():
        edge_zero(EDGE + tokens)

    chip_across = lax.div(across, 2)
    chip_ahead = lax.div(ahead, 2)
    chip_behind = lax.div(behind, 2)
    own_cols = pl.ds(pl.multiple_of(t * cols, cols), cols)

    with jax.named_scope('acti0'):
        activate(0)

    @pl.loop(1, span)
    def _(k):
        y_arrived(1, lax.rem(s + k, span))

    with jax.named_scope('giveacross0'):
        give(chip_across, 0)
    with jax.named_scope('acti1'):
        activate(1)
    with jax.named_scope('giveacross1'):
        give(chip_across, 1)
    with jax.named_scope('hop0across0'):
        hop(0, chip_across, 0)
    with jax.named_scope('giveahead0'):
        give(chip_ahead, 0)
    with jax.named_scope('hop0across1'):
        hop(0, chip_across, 1)
    with jax.named_scope('giveahead1'):
        give(chip_ahead, 1)
    with jax.named_scope('hop1behind0'):
        hop(1, chip_behind, 0)
    with jax.named_scope('givebehind0'):
        give(chip_behind, 0)
    with jax.named_scope('hop1behind1'):
        hop(1, chip_behind, 1)
    with jax.named_scope('givebehind1'):
        give(chip_behind, 1)
    with jax.named_scope('keep0'):
        held[0, lots[0]] = joined(chip_ahead, 0)
    with jax.named_scope('give0'):
        give(chip, 0)
    with jax.named_scope('keep1'):
        held[0, lots[1]] = joined(chip_ahead, 1)
    with jax.named_scope('give1'):
        give(chip, 1)
    for h in range(2):
        with jax.named_scope('hw0'):
            hop_copy(0, h).wait_recv()
        hop_out[2, lots[h]] = (held[0, lots[h]] + hop_in[0, lots[h]].astype(F32)).astype(BF16)
        hop_copy(2, h).start()
        own_normed = nx_buf[EDGE + h * mid : EDGE + (h + 1) * mid, own_cols].astype(F32)
        held[1, lots[h]] = joined(chip, h) + own_normed
    for h in range(2):
        with jax.named_scope('hw1'):
            hop_copy(1, h).wait_recv()
        with jax.named_scope('hw2'):
            hop_copy(2, h).wait_recv()
        terms = hop_in[1, lots[h]].astype(F32) + hop_in[2, lots[h]].astype(F32)
        out_buf[lots[h], :] = (held[1, lots[h]] + terms).astype(BF16)
        out_copy(h).start()

    for h in range(2):
        out_copy(h).wait()
    for way in range(2):
        kv_copy(way).wait_send()
        edge_copy(way).wait_send()
        for kind in range(2):
            for ab in range(2):
                n = half if ab == way else half - 1
                ref = (wide if kind == 0 else tall).at[0, pl.ds(0, n * depth), :]
                row = 2 * kind + ab
                remote(ref, ref, z_send.at[way, row], z_recv.at[row, 0], {"sp": right}).wait_send()
    for kind in range(2):
        ref = (wide if kind == 0 else tall).at[0, pl.ds(0, (span - 1) * depth), :]
        remote(ref, ref, y_send.at[kind], y_recv.at[kind, 0], {"grp": pair_grp}).wait_send()
        for slot in range(7):
            x_copy(kind, t, slot, partner).wait_send()
    for h in range(2):
        for owner in range(chips):
            pair_copy(owner, h).wait_send()
        for i in range(3):
            hop_copy(i, h).wait_send()


def solution(mesh):
    span, ranks = mesh.shape["sp"], mesh.shape["tp"]

    def shards(q, k, v, sink, resid, out_proj, gain, w_gate, w_up, conv_w, conv_b, w_down):
        tokens, width = resid.shape
        depth, hidden = w_gate.shape
        cols = width // ranks
        chips = ranks // 2
        pw, pd = 2 * hidden // 3, hidden // 3
        there = pl.BlockSpec(memory_space=pltpu.HBM)
        scalar = pl.BlockSpec(memory_space=pltpu.SMEM)
        dma = pltpu.SemaphoreType.DMA
        return pl.pallas_call(
            functools.partial(layer_kernel, span, ranks),
            out_shape=jax.ShapeDtypeStruct((tokens, cols), BF16),
            in_specs=[there, there, there, scalar] + [there] * 8,
            out_specs=there,
            scratch_shapes=[
                pltpu.VMEM((1, width), F32),
                pltpu.VMEM(conv_w.shape, F32),
                pltpu.VMEM(conv_b.shape, F32),
                pltpu.VMEM((tokens, HD), BF16),
                pltpu.VMEM((2, tokens + 2 * WINDOW, HD), BF16),
                pltpu.VMEM((tokens, width), BF16),
                pltpu.VMEM((ranks, out_proj.shape[0], cols), BF16),
                pltpu.VMEM((tokens, ranks * HD), BF16),
                pltpu.VMEM((tokens, width), F32),
                pltpu.VMEM((2, tokens, cols // 2), F32),
                pltpu.VMEM((tokens + 2 * EDGE, width), BF16),
                pltpu.VMEM((3, span * depth, pw), BF16),
                pltpu.VMEM((3, span * depth, pd), BF16),
                pltpu.VMEM((3, tokens + 2 * EDGE, pw), F32),
                pltpu.VMEM((tokens, hidden), BF16),
                pltpu.VMEM((chips, tokens, cols), BF16),
                pltpu.VMEM((chips, tokens, cols), BF16),
                pltpu.VMEM((3, tokens, cols), BF16),
                pltpu.VMEM((3, tokens, cols), BF16),
                pltpu.VMEM((2, tokens, cols), F32),
                pltpu.VMEM((tokens, cols), BF16),
                dma((2,)),
                dma((15,)),
                dma((2,)),
                dma((2,)),
                dma((2, 4)),
                dma((4, span)),
                dma((2,)),
                dma((2, span)),
                dma((2, 7)),
                dma((2, ranks)),
                dma((2,)),
                dma((2,)),
                dma((chips, 2)),
                dma((chips, 2)),
                dma((3, 2)),
                dma((3, 2)),
            ],
            compiler_params=pltpu.CompilerParams(
                collective_id=0, has_side_effects=True, vmem_limit_bytes=60 * 1024 * 1024
            ),
        )(
            q, k, v, sink, resid, out_proj, gain.reshape(1, width), w_gate, w_up,
            conv_w, conv_b, w_down.T,
        )

    return jax.shard_map(
        shards,
        mesh=mesh,
        in_specs=(
            P(("grp", "sp"), "tp"),
            P(("grp", "sp"), None),
            P(("grp", "sp"), None),
            P("tp"),
            P(("grp", "sp"), None),
            P(None, "tp"),
            P(),
            P("sp", "tp"),
            P("sp", "tp"),
            P(None, "tp"),
            P("tp"),
            P("tp", "sp"),
        ),
        out_specs=P(("grp", "sp"), "tp"),
        check_vma=False,
    )
```

```python
import functools

import jax
import jax.numpy as jnp
from jax import lax
from jax.experimental import pallas as pl
from jax.experimental.pallas import tpu as pltpu
from jax.sharding import PartitionSpec as P

H = 8
KVH = 2
HD = 128
WINDOW = 128
CONV = 3
EDGE = 16
MESH = pl.DeviceIdType.MESH
F32 = jnp.float32
BF16 = jnp.bfloat16


def layer_kernel(
    span,
    ranks,
    q_hbm,
    k_hbm,
    v_hbm,
    sink_ref,
    res_hbm,
    op_hbm,
    gain_hbm,
    wg_hbm,
    wu_hbm,
    cw_hbm,
    cb_hbm,
    wd_hbm,
    out_ref,
    gain_ref,
    cw_ref,
    cb_ref,
    q_buf,
    kv_buf,
    res_buf,
    op_buf,
    mix_buf,
    summed,
    stat,
    nx_buf,
    wide,
    tall,
    accs,
    act_buf,
    theirs_out,
    theirs_in,
    hop_out,
    hop_in,
    held,
    out_buf,
    out_sem,
    load_sem,
    kv_send,
    kv_recv,
    z_send,
    z_recv,
    y_send,
    y_recv,
    x_send,
    x_recv,
    edge_send,
    edge_recv,
    pair_send,
    pair_recv,
    hop_send,
    hop_recv,
):
    tokens, width = res_buf.shape
    depth, hidden = wg_hbm.shape
    cols = width // ranks
    half = span // 2
    pw = wide.shape[2]
    pd = tall.shape[2]
    chips = ranks // 2

    g = lax.axis_index("grp")
    s = lax.axis_index("sp")
    t = lax.axis_index("tp")
    right, left = lax.rem(s + 1, span), lax.rem(s + span - 1, span)
    parity = lax.rem(g, 2)
    pair_grp = g + 1 - 2 * parity
    own, other = 2 * parity, 2 - 2 * parity
    core = lax.rem(t, 2)
    chip = lax.div(t, 2)
    partner = t + 1 - 2 * core
    ahead = lax.rem(t + 2 - 4 * core + ranks, ranks)
    behind = lax.rem(t - 2 + 4 * core + ranks, ranks)
    across = lax.rem(t + ranks // 2, ranks)
    kv_col = pl.multiple_of(lax.div(t * KVH, ranks) * HD, HD)

    def scoped(name, fn):
        def run():
            with jax.named_scope(name):
                fn()

        return run

    def rows(j):
        return pl.ds(pl.multiple_of(j * depth, depth), depth)

    own_rows = rows(s)
    cut = pw - (hidden - pw)
    loads = [
        (wg_hbm.at[:, pl.ds(0, pw)], wide.at[0, own_rows, :]),
        (wg_hbm.at[:, pl.ds(pw, hidden - pw)], wide.at[1, own_rows, pl.ds(0, hidden - pw)]),
        (wu_hbm.at[:, pl.ds(0, cut)], wide.at[1, own_rows, pl.ds(hidden - pw, cut)]),
        (wu_hbm.at[:, pl.ds(cut, pw)], wide.at[2, own_rows, :]),
        (wd_hbm.at[:, pl.ds(0, pd)], tall.at[0, own_rows, :]),
        (wd_hbm.at[:, pl.ds(pd, pd)], tall.at[1, own_rows, :]),
        (wd_hbm.at[:, pl.ds(2 * pd, pd)], tall.at[2, own_rows, :]),
        (k_hbm.at[:, pl.ds(kv_col, HD)], kv_buf.at[0, pl.ds(WINDOW, tokens), :]),
        (v_hbm.at[:, pl.ds(kv_col, HD)], kv_buf.at[1, pl.ds(WINDOW, tokens), :]),
        (q_hbm, q_buf),
        (op_hbm, op_buf.at[t]),
        (res_hbm, res_buf),
        (gain_hbm, gain_ref),
        (cw_hbm, cw_ref),
        (cb_hbm, cb_ref),
    ]
    loads = [pltpu.make_async_copy(a, b, load_sem.at[i]) for i, (a, b) in enumerate(loads)]

    barrier = pltpu.get_barrier_semaphore()
    greeted = ({"sp": right}, {"sp": left}, {"grp": pair_grp}, {"tp": ahead}, {"tp": behind}, {"tp": partner})
    for who in greeted:
        pl.semaphore_signal(barrier, inc=1, device_id=who, device_id_type=MESH)
    for copy in loads:
        copy.start()

    def remote(src, dst, send, recv, who):
        return pltpu.make_async_remote_copy(
            src_ref=src, dst_ref=dst, send_sem=send, recv_sem=recv, device_id=who, device_id_type=MESH
        )

    def part(kind, index, j):
        return (wide if kind == 0 else tall).at[index, rows(j), :]

    def z_copy(kind, ab, j, way):
        ref = part(kind, own if ab else 1, j)
        row = 2 * kind + ab
        return remote(ref, ref, z_send.at[way, row], z_recv.at[row, j], {"sp": left if way else right})

    def y_copy(kind, j):
        ref = part(kind, own, j)
        return remote(ref, ref, y_send.at[kind], y_recv.at[kind, j], {"grp": pair_grp})

    def y_arrived(kind, j):
        ref = part(kind, other, j)
        remote(ref, ref, y_send.at[kind], y_recv.at[kind, j], {"grp": pair_grp}).wait_recv()

    def block(kind, b):
        if kind == 0:
            return op_buf.at[b]
        return mix_buf.at[:, pl.ds(pl.multiple_of(b * HD, HD), HD)]

    def x_copy(kind, b, slot, who):
        ref = block(kind, b)
        return remote(ref, ref, x_send.at[kind, slot], x_recv.at[kind, b], {"tp": who})

    def x_open(kind):
        x_copy(kind, t, 0, ahead).start()
        x_copy(kind, t, 1, behind).start()
        x_copy(kind, t, 2, partner).start()

    def x_pass(kind):
        x_copy(kind, behind, 3, ahead).wait_recv()
        x_copy(kind, behind, 3, ahead).start()
        x_copy(kind, behind, 4, partner).start()
        x_copy(kind, ahead, 5, partner).wait_recv()
        x_copy(kind, ahead, 5, partner).start()

    def x_last(kind):
        x_copy(kind, across, 6, partner).wait_recv()
        x_copy(kind, across, 6, partner).start()

    def x_close(kind):
        for step in range(chips):
            b = lax.rem(partner + 2 * step, ranks)
            x_copy(kind, b, 0, partner).wait_recv()

    def kv_copy(way):
        here, there = (tokens, 0) if way == 0 else (WINDOW, WINDOW + tokens)
        src, dst = kv_buf.at[core, pl.ds(here, WINDOW), :], kv_buf.at[core, pl.ds(there, WINDOW), :]
        return remote(src, dst, kv_send.at[way, 0], kv_recv.at[way, core], {"sp": left if way else right})

    def kv_hand(way, which):
        ref = kv_buf.at[which, pl.ds(WINDOW + tokens if way else 0, WINDOW), :]
        return remote(ref, ref, kv_send.at[way, 1], kv_recv.at[way, which], {"tp": partner})

    side = width // 2

    def edge_copy(way):
        here, there = (tokens, 0) if way == 0 else (EDGE, EDGE + tokens)
        lanes = pl.ds(pl.multiple_of(core * side, side), side)
        src, dst = nx_buf.at[pl.ds(here, EDGE), lanes], nx_buf.at[pl.ds(there, EDGE), lanes]
        return remote(src, dst, edge_send.at[way, 0], edge_recv.at[way, core], {"sp": left if way else right})

    def edge_hand(way, which):
        lanes = pl.ds(pl.multiple_of(which * side, side), side)
        ref = nx_buf.at[pl.ds(EDGE + tokens if way else 0, EDGE), lanes]
        return remote(ref, ref, edge_send.at[way, 1], edge_recv.at[way, which], {"tp": partner})

    def attend(i):
        lo = i * WINDOW
        keys = kv_buf[0, lo : lo + 3 * WINDOW, :]
        vals = kv_buf[1, lo : lo + 3 * WINDOW, :]
        scores = lax.dot_general(
            q_buf[lo : lo + WINDOW, :], keys, (((1,), (1,)), ((), ())), preferred_element_type=F32
        ) * (HD ** (-0.5))
        row = lax.broadcasted_iota(jnp.int32, scores.shape, 0)
        col = lax.broadcasted_iota(jnp.int32, scores.shape, 1)
        pos = s * tokens + (lo - WINDOW) + col
        gap = col - row
        seen = (gap >= 0) & (gap <= 2 * WINDOW) & (pos >= 0) & (pos < span * tokens)
        scores = jnp.where(seen, scores, F32(-1e30))
        sink = sink_ref[0]
        top = jnp.maximum(jnp.max(scores, axis=-1, keepdims=True), sink)
        expo = jnp.exp(scores - top)
        total = jnp.sum(expo, axis=-1, keepdims=True) + jnp.exp(sink - top)
        weights = (expo / total).astype(BF16)
        mixed = jnp.dot(weights, vals, preferred_element_type=F32).astype(BF16)
        mix_buf[lo : lo + WINDOW, pl.ds(pl.multiple_of(t * HD, HD), HD)] = mixed

    def project(o, opens):
        at = pl.ds(pl.multiple_of(o * cols, cols), cols)
        block_sum = res_buf[:, at].astype(F32) + jnp.dot(mix_buf[...], op_buf[o], preferred_element_type=F32)
        summed[:, at] = block_sum
        first, second = block_sum[:, : cols // 2], block_sum[:, cols // 2 :]
        lone = first + second
        squares = first * first + second * second
        if opens:
            stat[0] = lone
            stat[1] = squares
        else:
            stat[0] += lone
            stat[1] += squares

    def normalize(lo, hi):
        @pl.loop(lo // EDGE, hi // EDGE)
        def _(i):
            at = pl.ds(pl.multiple_of(i * EDGE, EDGE), EDGE)
            mean = jnp.sum(stat[0, at, :], axis=-1, keepdims=True) / width
            msq = jnp.sum(stat[1, at, :], axis=-1, keepdims=True) / width
            scale = lax.rsqrt(msq - mean * mean + 1e-05)
            normed = (summed[at, :] - mean) * scale * gain_ref[...]
            nx_buf[pl.ds(pl.multiple_of(i * EDGE + EDGE, EDGE), EDGE), :] = normed.astype(BF16)

    mid = tokens // 2
    lots = [slice(0, mid), slice(mid, tokens)]
    quads = span * depth // cols
    mine = lax.div(s * depth, cols)

    def gates(shift, first=False):
        quad = lax.rem(mine + shift + quads, quads)
        for i in range(cols // depth):
            j = quad * (cols // depth) + i

            @pl.when(j != s)
            def _():
                y_arrived(0, j)

        at = pl.ds(pl.multiple_of(quad * cols, cols), cols)
        x = nx_buf[:, at]
        for p in range(3):
            y = jnp.dot(x, wide[p, at, :], preferred_element_type=F32)
            if first:
                accs[p] = y
            else:
                accs[p] += y

    def edge_zero(where):
        for p in range(2):
            accs[p, where : where + EDGE, :] = jnp.zeros((EDGE, pw), F32)

    def activate(half_of):
        for h in range(3):
            gp, gc = divmod(h * pd, pw)
            up, uc = divmod(hidden + h * pd, pw)
            for r in range(half_of * mid, (half_of + 1) * mid, WINDOW):
                conv = cb_ref[h * pd : (h + 1) * pd].reshape(1, pd)
                for tap in range(CONV):
                    lo = EDGE - CONV // 2 + tap + r
                    gate = accs[gp, lo : lo + WINDOW, gc : gc + pd].astype(BF16).astype(F32)
                    conv = conv + gate * cw_ref[tap : tap + 1, h * pd : (h + 1) * pd]
                ups = accs[up, EDGE + r : EDGE + r + WINDOW, uc : uc + pd].astype(BF16).astype(F32)
                act = conv / (1.0 + jnp.exp(-conv)) * ups
                act_buf[r : r + WINDOW, h * pd : (h + 1) * pd] = act.astype(BF16)

    def partial(o, h):
        lot = lots[h]
        if h == 0:
            for i in range(cols // depth):
                j = o * (cols // depth) + i

                @pl.when(j != s)
                def _():
                    y_arrived(1, j)

        at = pl.ds(pl.multiple_of(o * cols, cols), cols)
        total = None
        for p in range(3):
            term = lax.dot_general(
                act_buf[lot, p * pd : (p + 1) * pd],
                tall[p, at, :],
                (((1,), (1,)), ((), ())),
                preferred_element_type=F32,
            )
            total = term if total is None else total + term
        return total

    def pair_copy(owner, h):
        src, dst = theirs_out.at[owner, lots[h]], theirs_in.at[owner, lots[h]]
        return remote(src, dst, pair_send.at[owner, h], pair_recv.at[owner, h], {"tp": partner})

    def hop_copy(i, h):
        src, dst = hop_out.at[i, lots[h]], hop_in.at[i, lots[h]]
        return remote(src, dst, hop_send.at[i, h], hop_recv.at[i, h], {"tp": behind if i == 1 else ahead})

    def out_copy(h):
        return pltpu.make_async_copy(out_buf.at[lots[h], :], out_ref.at[lots[h], :], out_sem.at[h])

    def give(owner, h):
        theirs_out[owner, lots[h]] = partial(2 * owner + 1 - core, h).astype(BF16)
        pair_copy(owner, h).start()

    def joined(owner, h):
        kept = partial(2 * owner + core, h)
        pair_copy(owner, h).wait_recv()
        return kept + theirs_in[owner, lots[h]].astype(F32)

    def hop(i, owner, h):
        hop_out[i, lots[h]] = joined(owner, h).astype(BF16)
        hop_copy(i, h).start()

    with jax.named_scope('load'):
        for i in range(9):
            loads[i].wait()
    with jax.named_scope('bar'):
        pl.semaphore_wait(barrier, len(greeted))
    for kind in range(2):
        for turn in range(2):
            for way in range(2):
                z_copy(kind, turn if way == 0 else 1 - turn, s, way).start()
        if kind == 0:
            for way in range(2):
                kv_copy(way).start()
    loads[10].wait()
    x_open(0)
    loads[9].wait()

    blocks = tokens // WINDOW

    def unit_attend(inner):
        if inner:
            for way in range(2):
                kv_copy(way).wait_recv()
                kv_hand(way, core).start()
            for i in range(1, blocks - 1):
                attend(i)
        else:
            for way in range(2):
                kv_hand(way, 1 - core).wait_recv()
            attend(0)
            attend(blocks - 1)
            x_open(1)

    def unit_edge():
        unit_normalize(2)
        for way in range(2):
            edge_copy(way).wait_recv()
            edge_hand(way, core).start()

    def mirror(b):
        return b + 1 - 2 * lax.rem(b, 2)

    def unit_project(stage):
        if stage == 0:
            x_close(1)
            for i in range(11, 15):
                loads[i].wait()
            project(t, True)
            project(ahead, False)
        if stage == 1:
            x_last(0)
            x_copy(0, partner, 0, partner).wait_recv()
            project(behind, False)
            project(partner, False)
        if stage == 2:
            for b in (mirror(ahead), mirror(behind)):
                x_copy(0, b, 0, partner).wait_recv()
                project(b, False)
        if stage == 3:
            x_copy(0, mirror(across), 0, partner).wait_recv()
            project(across, False)
            project(mirror(across), False)

    quarter = tokens // 4

    def unit_normalize(i, send=False):
        normalize(i * quarter, (i + 1) * quarter)
        if send:
            for way in range(2):
                edge_copy(way).start()

    def unit_gates(shifts, first=False):
        if first:
            for way in range(2):
                edge_hand(way, 1 - core).wait_recv()
        for i, shift in enumerate(shifts):
            gates(shift, first and i == 0)

    units = {
        (1, 0): lambda: unit_attend(True),
        (1, 1): lambda: unit_attend(False),
        (3, 0): lambda: x_pass(0),
        (3, 1): lambda: x_pass(1),
        (5, 0): lambda: x_last(1),
        (6, 0): lambda: unit_project(0),
        (6, 1): lambda: unit_project(1),
        (7, 0): lambda: unit_project(2),
        (7, 1): lambda: unit_project(3),
        (8, 0): lambda: unit_normalize(0),
        (8, 1): lambda: unit_normalize(3, True),
        (9, 0): lambda: unit_normalize(1),
        (9, 1): unit_edge,
        (10, 0): lambda: unit_gates([0], True),
        (10, 1): lambda: unit_gates([1]),
        (11, 0): lambda: unit_gates([-1]),
        (12, 1): lambda: unit_gates([2]),
        (13, 0): lambda: unit_gates([-2]),
    }

    def hop_on(kind, k, swap):
        back = lax.rem(s - k + span, span)
        front = lax.rem(s + k, span)
        for turn in range(2):
            for way, j in ((0, back), (1, front)):
                ab = turn if way == 0 else 1 - turn
                z_copy(kind, ab, j, way).wait_recv()
                if ab == way:
                    z_copy(kind, ab, j, way).start()
                else:

                    @pl.when(k < half - 1)
                    def _():
                        z_copy(kind, ab, j, way).start()

                if ab == 1 and swap is not False:
                    pl.when(swap)(y_copy(kind, j).start)

    def swap_down(k):
        y_copy(1, lax.rem(s - k + span, span)).start()
        y_copy(1, lax.rem(s + k, span)).start()

    def ring_wide(k):
        with jax.named_scope('hop0'):
            hop_on(0, k, True)

    def ring_tall(k):
        with jax.named_scope('hop1'):
            hop_on(1, k - 1, False if k is half else k < half - 1)

    @pl.loop(1, half)
    def _(k):
        ring_wide(k)
        for (step, slot), unit in units.items():
            if slot == 0:
                pl.when(k == step)(unit)

        @pl.when(k > 1)
        def _():
            ring_tall(k)

        for (step, slot), unit in units.items():
            if slot == 1:
                pl.when(k == step)(unit)

    far = lax.rem(s + half, span)
    with jax.named_scope('far0b'):
        z_copy(0, 1, far, 1).wait_recv()
    y_copy(0, far).start()
    with jax.named_scope('far0a'):
        z_copy(0, 0, far, 0).wait_recv()
    swap_down(half - 2)
    ring_tall(half)
    swap_down(half - 1)

    with jax.named_scope('gate3'):
        gates(3)
    with jax.named_scope('gate3'):
        gates(-3)
    with jax.named_scope('gate4'):
        gates(4)

    @pl.when(s == 0)
    def _():
        edge_zero(0)

    @pl.when(s == span - 1)
    def _():
        edge_zero(EDGE + tokens)

    chip_across = lax.div(across, 2)
    chip_ahead = lax.div(ahead, 2)
    chip_behind = lax.div(behind, 2)
    own_cols = pl.ds(pl.multiple_of(t * cols, cols), cols)

    with jax.named_scope('acti0'):
        activate(0)
    with jax.named_scope('far1b'):
        z_copy(1, 1, far, 1).wait_recv()
    y_copy(1, far).start()
    with jax.named_scope('far1a'):
        z_copy(1, 0, far, 0).wait_recv()
    with jax.named_scope('giveacross0'):
        give(chip_across, 0)
    with jax.named_scope('acti1'):
        activate(1)
    with jax.named_scope('giveacross1'):
        give(chip_across, 1)
    with jax.named_scope('hop0across0'):
        hop(0, chip_across, 0)
    with jax.named_scope('giveahead0'):
        give(chip_ahead, 0)
    with jax.named_scope('hop0across1'):
        hop(0, chip_across, 1)
    with jax.named_scope('giveahead1'):
        give(chip_ahead, 1)
    with jax.named_scope('hop1behind0'):
        hop(1, chip_behind, 0)
    with jax.named_scope('givebehind0'):
        give(chip_behind, 0)
    with jax.named_scope('hop1behind1'):
        hop(1, chip_behind, 1)
    with jax.named_scope('givebehind1'):
        give(chip_behind, 1)
    with jax.named_scope('keep0'):
        held[0, lots[0]] = joined(chip_ahead, 0)
    with jax.named_scope('give0'):
        give(chip, 0)
    with jax.named_scope('keep1'):
        held[0, lots[1]] = joined(chip_ahead, 1)
    with jax.named_scope('give1'):
        give(chip, 1)
    for h in range(2):
        with jax.named_scope('hw0'):
            hop_copy(0, h).wait_recv()
        hop_out[2, lots[h]] = (held[0, lots[h]] + hop_in[0, lots[h]].astype(F32)).astype(BF16)
        hop_copy(2, h).start()
        own_normed = nx_buf[EDGE + h * mid : EDGE + (h + 1) * mid, own_cols].astype(F32)
        held[1, lots[h]] = joined(chip, h) + own_normed
    for h in range(2):
        with jax.named_scope('hw1'):
            hop_copy(1, h).wait_recv()
        with jax.named_scope('hw2'):
            hop_copy(2, h).wait_recv()
        terms = hop_in[1, lots[h]].astype(F32) + hop_in[2, lots[h]].astype(F32)
        out_buf[lots[h], :] = (held[1, lots[h]] + terms).astype(BF16)
        out_copy(h).start()

    with jax.named_scope('outw'):
        for h in range(2):
            out_copy(h).wait()
    with jax.named_scope('sent'):
        for way in range(2):
            kv_copy(way).wait_send()
            kv_hand(way, core).wait_send()
            edge_copy(way).wait_send()
            edge_hand(way, core).wait_send()
            for kind in range(2):
                for ab in range(2):
                    n = half if ab == way else half - 1
                    ref = (wide if kind == 0 else tall).at[0, pl.ds(0, n * depth), :]
                    row = 2 * kind + ab
                    remote(ref, ref, z_send.at[way, row], z_recv.at[row, 0], {"sp": right}).wait_send()
        for kind in range(2):
            ref = (wide if kind == 0 else tall).at[0, pl.ds(0, (span - 1) * depth), :]
            remote(ref, ref, y_send.at[kind], y_recv.at[kind, 0], {"grp": pair_grp}).wait_send()
            for slot in range(7):
                x_copy(kind, t, slot, partner).wait_send()
        for h in range(2):
            for owner in range(chips):
                pair_copy(owner, h).wait_send()
            for i in range(3):
                hop_copy(i, h).wait_send()


def solution(mesh):
    span, ranks = mesh.shape["sp"], mesh.shape["tp"]

    def shards(q, k, v, sink, resid, out_proj, gain, w_gate, w_up, conv_w, conv_b, w_down):
        tokens, width = resid.shape
        depth, hidden = w_gate.shape
        cols = width // ranks
        chips = ranks // 2
        pw, pd = 2 * hidden // 3, hidden // 3
        there = pl.BlockSpec(memory_space=pltpu.HBM)
        scalar = pl.BlockSpec(memory_space=pltpu.SMEM)
        dma = pltpu.SemaphoreType.DMA
        return pl.pallas_call(
            functools.partial(layer_kernel, span, ranks),
            out_shape=jax.ShapeDtypeStruct((tokens, cols), BF16),
            in_specs=[there, there, there, scalar] + [there] * 8,
            out_specs=there,
            scratch_shapes=[
                pltpu.VMEM((1, width), F32),
                pltpu.VMEM(conv_w.shape, F32),
                pltpu.VMEM(conv_b.shape, F32),
                pltpu.VMEM((tokens, HD), BF16),
                pltpu.VMEM((2, tokens + 2 * WINDOW, HD), BF16),
                pltpu.VMEM((tokens, width), BF16),
                pltpu.VMEM((ranks, out_proj.shape[0], cols), BF16),
                pltpu.VMEM((tokens, ranks * HD), BF16),
                pltpu.VMEM((tokens, width), F32),
                pltpu.VMEM((2, tokens, cols // 2), F32),
                pltpu.VMEM((tokens + 2 * EDGE, width), BF16),
                pltpu.VMEM((3, span * depth, pw), BF16),
                pltpu.VMEM((3, span * depth, pd), BF16),
                pltpu.VMEM((3, tokens + 2 * EDGE, pw), F32),
                pltpu.VMEM((tokens, hidden), BF16),
                pltpu.VMEM((chips, tokens, cols), BF16),
                pltpu.VMEM((chips, tokens, cols), BF16),
                pltpu.VMEM((3, tokens, cols), BF16),
                pltpu.VMEM((3, tokens, cols), BF16),
                pltpu.VMEM((2, tokens, cols), F32),
                pltpu.VMEM((tokens, cols), BF16),
                dma((2,)),
                dma((15,)),
                dma((2, 2)),
                dma((2, 2)),
                dma((2, 4)),
                dma((4, span)),
                dma((2,)),
                dma((2, span)),
                dma((2, 7)),
                dma((2, ranks)),
                dma((2, 2)),
                dma((2, 2)),
                dma((chips, 2)),
                dma((chips, 2)),
                dma((3, 2)),
                dma((3, 2)),
            ],
            compiler_params=pltpu.CompilerParams(
                collective_id=0, has_side_effects=True, vmem_limit_bytes=60 * 1024 * 1024
            ),
        )(
            q, k, v, sink, resid, out_proj, gain.reshape(1, width), w_gate, w_up,
            conv_w, conv_b, w_down.T,
        )

    return jax.shard_map(
        shards,
        mesh=mesh,
        in_specs=(
            P(("grp", "sp"), "tp"),
            P(("grp", "sp"), None),
            P(("grp", "sp"), None),
            P("tp"),
            P(("grp", "sp"), None),
            P(None, "tp"),
            P(),
            P("sp", "tp"),
            P("sp", "tp"),
            P(None, "tp"),
            P("tp"),
            P("tp", "sp"),
        ),
        out_specs=P(("grp", "sp"), "tp"),
        check_vma=False,
    )
```

```python
import functools

import jax
import jax.numpy as jnp
from jax import lax
from jax.experimental import pallas as pl
from jax.experimental.pallas import tpu as pltpu
from jax.sharding import PartitionSpec as P

H = 8
KVH = 2
HD = 128
WINDOW = 128
CONV = 3
EDGE = 16
MESH = pl.DeviceIdType.MESH
F32 = jnp.float32
BF16 = jnp.bfloat16


def layer_kernel(
    span,
    ranks,
    q_hbm,
    k_hbm,
    v_hbm,
    sink_ref,
    res_hbm,
    op_hbm,
    gain_hbm,
    wg_hbm,
    wu_hbm,
    cw_hbm,
    cb_hbm,
    wd_hbm,
    out_ref,
    gain_ref,
    cw_ref,
    cb_ref,
    q_buf,
    kv_buf,
    res_buf,
    op_buf,
    mix_buf,
    summed,
    stat,
    nx_buf,
    wide,
    tall,
    accs,
    act_buf,
    theirs_out,
    theirs_in,
    hop_out,
    hop_in,
    held,
    out_buf,
    out_sem,
    load_sem,
    kv_send,
    kv_recv,
    z_send,
    z_recv,
    y_send,
    y_recv,
    x_send,
    x_recv,
    edge_send,
    edge_recv,
    pair_send,
    pair_recv,
    hop_send,
    hop_recv,
):
    tokens, width = res_buf.shape
    depth, hidden = wg_hbm.shape
    cols = width // ranks
    quad_of = cols // depth
    half = span // 2
    pw = wide.shape[2]
    pd = tall.shape[2]
    chips = ranks // 2

    g = lax.axis_index("grp")
    s = lax.axis_index("sp")
    t = lax.axis_index("tp")
    right, left = lax.rem(s + 1, span), lax.rem(s + span - 1, span)
    parity = lax.rem(g, 2)
    pair_grp = g + 1 - 2 * parity
    own, other = 2 * parity, 2 - 2 * parity
    core = lax.rem(t, 2)
    chip = lax.div(t, 2)
    partner = t + 1 - 2 * core
    ahead = lax.rem(t + 2 - 4 * core + ranks, ranks)
    behind = lax.rem(t - 2 + 4 * core + ranks, ranks)
    across = lax.rem(t + ranks // 2, ranks)
    kv_col = pl.multiple_of(lax.div(t * KVH, ranks) * HD, HD)

    def scoped(name, fn):
        def run():
            with jax.named_scope(name):
                fn()

        return run

    def rows(j):
        return pl.ds(pl.multiple_of(j * depth, depth), depth)

    own_rows = rows(s)
    cut = pw - (hidden - pw)
    def own_copies(sem, pairs):
        return [pltpu.make_async_copy(src, dst, load_sem.at[sem]) for src, dst in pairs]

    def loaded(sem, ref):
        pltpu.make_async_copy(ref, ref, load_sem.at[sem]).wait()

    rest = hidden - pw
    loads = own_copies(
        0,
        [
            (wg_hbm.at[:, pl.ds(0, pw)], wide.at[0, own_rows, :]),
            (wg_hbm.at[:, pl.ds(pw, rest)], wide.at[1, own_rows, pl.ds(0, rest)]),
            (wu_hbm.at[:, pl.ds(0, cut)], wide.at[1, own_rows, pl.ds(rest, cut)]),
            (wu_hbm.at[:, pl.ds(cut, pw)], wide.at[2, own_rows, :]),
        ],
    )
    loads += own_copies(1, [(wd_hbm.at[:, pl.ds(p * pd, pd)], tall.at[p, own_rows, :]) for p in range(3)])
    loads += own_copies(
        2,
        [
            (k_hbm.at[:, pl.ds(kv_col, HD)], kv_buf.at[0, pl.ds(WINDOW, tokens), :]),
            (v_hbm.at[:, pl.ds(kv_col, HD)], kv_buf.at[1, pl.ds(WINDOW, tokens), :]),
        ],
    )
    small = [(q_hbm, q_buf), (op_hbm, op_buf.at[t]), (res_hbm, res_buf), (gain_hbm, gain_ref), (cw_hbm, cw_ref), (cb_hbm, cb_ref)]
    single = [own_copies(3 + i, [pair])[0] for i, pair in enumerate(small)]
    loads += single

    barrier = pltpu.get_barrier_semaphore()
    greeted = ({"sp": right}, {"sp": left}, {"grp": pair_grp}, {"tp": ahead}, {"tp": behind}, {"tp": partner})
    for who in greeted:
        pl.semaphore_signal(barrier, inc=1, device_id=who, device_id_type=MESH)
    for copy in loads:
        copy.start()

    def remote(src, dst, send, recv, who):
        return pltpu.make_async_remote_copy(
            src_ref=src, dst_ref=dst, send_sem=send, recv_sem=recv, device_id=who, device_id_type=MESH
        )

    def part(kind, index, j):
        return (wide if kind == 0 else tall).at[index, rows(j), :]

    def z_copy(kind, ab, j, way, turns):
        ref = part(kind, own if ab else 1, j)
        row = 2 * kind + ab
        recv = z_recv.at[way, row, lax.rem(turns, 4)]
        return remote(ref, ref, z_send.at[way, row], recv, {"sp": left if way else right})

    def y_copy(kind, j):
        ref = part(kind, own, j)
        return remote(ref, ref, y_send.at[kind], y_recv.at[kind, lax.div(j, quad_of)], {"grp": pair_grp})

    def y_arrived(kind, quad):
        def wait(n):
            buf = wide if kind == 0 else tall
            ref = buf.at[other, pl.ds(pl.multiple_of(quad * cols, cols), n * depth), :]
            remote(ref, ref, y_send.at[kind], y_recv.at[kind, quad], {"grp": pair_grp}).wait_recv()

        is_own = quad == lax.div(s, quad_of)

        @pl.when(is_own)
        def _():
            wait(quad_of - 1)

        @pl.when(jnp.logical_not(is_own))
        def _():
            wait(quad_of)

    def block(kind, b):
        if kind == 0:
            return op_buf.at[b]
        return mix_buf.at[:, pl.ds(pl.multiple_of(b * HD, HD), HD)]

    def x_copy(kind, b, slot, who):
        ref = block(kind, b)
        return remote(ref, ref, x_send.at[kind], x_recv.at[kind, b], {"tp": who})

    def x_open(kind):
        x_copy(kind, t, 0, ahead).start()
        x_copy(kind, t, 1, behind).start()
        x_copy(kind, t, 2, partner).start()

    def x_pass(kind):
        x_copy(kind, behind, 3, ahead).wait_recv()
        x_copy(kind, behind, 3, ahead).start()
        x_copy(kind, behind, 4, partner).start()
        x_copy(kind, ahead, 5, partner).wait_recv()
        x_copy(kind, ahead, 5, partner).start()

    def x_last(kind):
        x_copy(kind, across, 6, partner).wait_recv()
        x_copy(kind, across, 6, partner).start()

    def x_close(kind):
        for step in range(chips):
            b = lax.rem(partner + 2 * step, ranks)
            x_copy(kind, b, 0, partner).wait_recv()

    def kv_copy(way):
        here, there = (tokens, 0) if way == 0 else (WINDOW, WINDOW + tokens)
        src, dst = kv_buf.at[core, pl.ds(here, WINDOW), :], kv_buf.at[core, pl.ds(there, WINDOW), :]
        return remote(src, dst, kv_send, kv_recv.at[way, core], {"sp": left if way else right})

    def kv_hand(way, which):
        ref = kv_buf.at[which, pl.ds(WINDOW + tokens if way else 0, WINDOW), :]
        return remote(ref, ref, kv_send, kv_recv.at[way, which], {"tp": partner})

    side = width // 2

    def edge_copy(way):
        here, there = (tokens, 0) if way == 0 else (EDGE, EDGE + tokens)
        lanes = pl.ds(pl.multiple_of(core * side, side), side)
        src, dst = nx_buf.at[pl.ds(here, EDGE), lanes], nx_buf.at[pl.ds(there, EDGE), lanes]
        return remote(src, dst, edge_send, edge_recv.at[way, core], {"sp": left if way else right})

    def edge_hand(way, which):
        lanes = pl.ds(pl.multiple_of(which * side, side), side)
        ref = nx_buf.at[pl.ds(EDGE + tokens if way else 0, EDGE), lanes]
        return remote(ref, ref, edge_send, edge_recv.at[way, which], {"tp": partner})

    def attend(i):
        lo = i * WINDOW
        keys = kv_buf[0, lo : lo + 3 * WINDOW, :]
        vals = kv_buf[1, lo : lo + 3 * WINDOW, :]
        scores = lax.dot_general(
            q_buf[lo : lo + WINDOW, :], keys, (((1,), (1,)), ((), ())), preferred_element_type=F32
        ) * (HD ** (-0.5))
        row = lax.broadcasted_iota(jnp.int32, scores.shape, 0)
        col = lax.broadcasted_iota(jnp.int32, scores.shape, 1)
        pos = s * tokens + (lo - WINDOW) + col
        gap = col - row
        seen = (gap >= 0) & (gap <= 2 * WINDOW) & (pos >= 0) & (pos < span * tokens)
        scores = jnp.where(seen, scores, F32(-1e30))
        sink = sink_ref[0]
        top = jnp.maximum(jnp.max(scores, axis=-1, keepdims=True), sink)
        expo = jnp.exp(scores - top)
        total = jnp.sum(expo, axis=-1, keepdims=True) + jnp.exp(sink - top)
        weights = (expo / total).astype(BF16)
        mixed = jnp.dot(weights, vals, preferred_element_type=F32).astype(BF16)
        mix_buf[lo : lo + WINDOW, pl.ds(pl.multiple_of(t * HD, HD), HD)] = mixed

    def project(o, opens):
        at = pl.ds(pl.multiple_of(o * cols, cols), cols)
        block_sum = res_buf[:, at].astype(F32) + jnp.dot(mix_buf[...], op_buf[o], preferred_element_type=F32)
        summed[:, at] = block_sum
        first, second = block_sum[:, : cols // 2], block_sum[:, cols // 2 :]
        lone = first + second
        squares = first * first + second * second
        if opens:
            stat[0] = lone
            stat[1] = squares
        else:
            stat[0] += lone
            stat[1] += squares

    def normalize(lo, hi):
        @pl.loop(lo // EDGE, hi // EDGE)
        def _(i):
            at = pl.ds(pl.multiple_of(i * EDGE, EDGE), EDGE)
            mean = jnp.sum(stat[0, at, :], axis=-1, keepdims=True) / width
            msq = jnp.sum(stat[1, at, :], axis=-1, keepdims=True) / width
            scale = lax.rsqrt(msq - mean * mean + 1e-05)
            normed = (summed[at, :] - mean) * scale * gain_ref[...]
            nx_buf[pl.ds(pl.multiple_of(i * EDGE + EDGE, EDGE), EDGE), :] = normed.astype(BF16)

    mid = tokens // 2
    lots = [slice(0, mid), slice(mid, tokens)]
    parcels = [slice(q * tokens // 4, (q + 1) * tokens // 4) for q in range(4)]
    quads = span * depth // cols
    mine = lax.div(s * depth, cols)

    def gates(shift, first=False):
        quad = lax.rem(mine + shift + quads, quads)
        y_arrived(0, quad)
        at = pl.ds(pl.multiple_of(quad * cols, cols), cols)
        x = nx_buf[:, at]
        for p in range(3):
            y = jnp.dot(x, wide[p, at, :], preferred_element_type=F32)
            if first:
                accs[p] = y
            else:
                accs[p] += y

    def edge_zero(where):
        for p in range(2):
            accs[p, where : where + EDGE, :] = jnp.zeros((EDGE, pw), F32)

    def activate(half_of):
        for h in range(3):
            gp, gc = divmod(h * pd, pw)
            up, uc = divmod(hidden + h * pd, pw)
            for r in range(half_of * mid, (half_of + 1) * mid, WINDOW):
                conv = cb_ref[h * pd : (h + 1) * pd].reshape(1, pd)
                for tap in range(CONV):
                    lo = EDGE - CONV // 2 + tap + r
                    gate = accs[gp, lo : lo + WINDOW, gc : gc + pd].astype(BF16).astype(F32)
                    conv = conv + gate * cw_ref[tap : tap + 1, h * pd : (h + 1) * pd]
                ups = accs[up, EDGE + r : EDGE + r + WINDOW, uc : uc + pd].astype(BF16).astype(F32)
                act = conv / (1.0 + jnp.exp(-conv)) * ups
                act_buf[r : r + WINDOW, h * pd : (h + 1) * pd] = act.astype(BF16)

    def partial(o, h):
        lot = lots[h]
        if h == 0:
            y_arrived(1, o)

        at = pl.ds(pl.multiple_of(o * cols, cols), cols)
        total = None
        for p in range(3):
            term = lax.dot_general(
                act_buf[lot, p * pd : (p + 1) * pd],
                tall[p, at, :],
                (((1,), (1,)), ((), ())),
                preferred_element_type=F32,
            )
            total = term if total is None else total + term
        return total

    def pair_copy(owner, h):
        src, dst = theirs_out.at[owner, lots[h]], theirs_in.at[owner, lots[h]]
        return remote(src, dst, pair_send, pair_recv.at[owner, h], {"tp": partner})

    def hop_copy(i, q):
        src, dst = hop_out.at[i, parcels[q]], hop_in.at[i, parcels[q]]
        return remote(src, dst, hop_send, hop_recv.at[i, q], {"tp": behind if i == 1 else ahead})

    def out_copy(q):
        return pltpu.make_async_copy(out_buf.at[parcels[q], :], out_ref.at[parcels[q], :], out_sem)

    def give(owner, h):
        theirs_out[owner, lots[h]] = partial(2 * owner + 1 - core, h).astype(BF16)
        pair_copy(owner, h).start()

    def joined(owner, h):
        kept = partial(2 * owner + core, h)
        pair_copy(owner, h).wait_recv()
        return kept + theirs_in[owner, lots[h]].astype(F32)

    def hop(i, owner, h):
        hop_out[i, lots[h]] = joined(owner, h).astype(BF16)
        hop_copy(i, 2 * h).start()
        hop_copy(i, 2 * h + 1).start()

    blocks = tokens // WINDOW

    def attend_inner():
        for i in range(1, blocks - 1):
            attend(i)

    def unit_attend(inner):
        if inner:
            for way in range(2):
                kv_copy(way).wait_recv()
                kv_hand(way, core).start()
            pl.when(core == 0)(attend_inner)
        else:
            for way in range(2):
                kv_hand(way, 1 - core).wait_recv()
            attend(0)
            attend(blocks - 1)
            x_open(1)

    def unit_edge():
        unit_normalize(2)
        for way in range(2):
            edge_copy(way).wait_recv()
            edge_hand(way, core).start()

    def mirror(b):
        return b + 1 - 2 * lax.rem(b, 2)

    def unit_project(stage):
        if stage == 0:
            x_close(1)
            for copy in single[2:]:
                copy.wait()
            project(t, True)
            project(ahead, False)
        if stage == 1:
            x_last(0)
            x_copy(0, partner, 0, partner).wait_recv()
            project(behind, False)
            project(partner, False)
        if stage == 2:
            for b in (mirror(ahead), mirror(behind)):
                x_copy(0, b, 0, partner).wait_recv()
                project(b, False)
        if stage == 3:
            x_copy(0, mirror(across), 0, partner).wait_recv()
            project(across, False)
            project(mirror(across), False)

    quarter = tokens // 4

    def unit_normalize(i, send=False):
        normalize(i * quarter, (i + 1) * quarter)
        if send:
            for way in range(2):
                edge_copy(way).start()

    def unit_gates(shifts, first=False):
        if first:
            for way in range(2):
                edge_hand(way, 1 - core).wait_recv()
        for i, shift in enumerate(shifts):
            gates(shift, first and i == 0)

    loaded(0, wide.at[:, own_rows, :])
    loaded(1, tall.at[:, own_rows, :])
    loaded(2, kv_buf.at[:, pl.ds(WINDOW, tokens), :])
    single[0].wait()
    with jax.named_scope('bar'):
        pl.semaphore_wait(barrier, len(greeted))

    @pl.when(core == 1)
    def _():
        attend_inner()

    for kind in range(2):
        for turn in range(2):
            for way in range(2):
                z_copy(kind, turn if way == 0 else 1 - turn, s, way, 1).start()
        if kind == 0:
            for way in range(2):
                kv_copy(way).start()
    single[1].wait()
    x_open(0)

    units = {
        (1, 0): lambda: unit_attend(True),
        (1, 1): lambda: unit_attend(False),
        (3, 0): lambda: x_pass(0),
        (3, 1): lambda: x_pass(1),
        (5, 0): lambda: x_last(1),
        (6, 0): lambda: unit_project(0),
        (6, 1): lambda: unit_project(1),
        (7, 0): lambda: unit_project(2),
        (7, 1): lambda: unit_project(3),
        (8, 0): lambda: unit_normalize(0),
        (8, 1): lambda: unit_normalize(3, True),
        (9, 0): lambda: unit_normalize(1),
        (9, 1): unit_edge,
        (10, 0): lambda: unit_gates([0], True),
        (10, 1): lambda: unit_gates([1]),
        (11, 0): lambda: unit_gates([-1]),
        (12, 1): lambda: unit_gates([2]),
        (13, 0): lambda: unit_gates([-2]),
    }

    def hop_on(kind, k, swap, turns=(0, 1)):
        back = lax.rem(s - k + span, span)
        front = lax.rem(s + k, span)
        for turn in turns:
            for way, j in ((0, back), (1, front)):
                ab = turn if way == 0 else 1 - turn
                z_copy(kind, ab, j, way, k).wait_recv()
                if ab == way:
                    z_copy(kind, ab, j, way, k + 1).start()
                else:

                    @pl.when(k < half - 1)
                    def _():
                        z_copy(kind, ab, j, way, k + 1).start()

                if ab == 1 and swap is not False:
                    pl.when(swap)(y_copy(kind, j).start)

    def swap_down(k):
        y_copy(1, lax.rem(s - k + span, span)).start()
        y_copy(1, lax.rem(s + k, span)).start()

    def ring_wide(k):
        with jax.named_scope('hop0'):
            hop_on(0, k, True)

    def ring_tall(k):
        hop_on(1, k - 1, k < half - 1)

    @pl.loop(1, half)
    def _(k):
        ring_wide(k)
        for (step, slot), unit in units.items():
            if slot == 0:
                pl.when(k == step)(unit)

        @pl.when(k > 1)
        def _():
            ring_tall(k)

        for (step, slot), unit in units.items():
            if slot == 1:
                pl.when(k == step)(unit)

    far = lax.rem(s + half, span)
    with jax.named_scope('far0b'):
        z_copy(0, 1, far, 1, half).wait_recv()
    y_copy(0, far).start()
    with jax.named_scope('far0a'):
        z_copy(0, 0, far, 0, half).wait_recv()
    swap_down(half - 2)

    with jax.named_scope('gate3'):
        gates(3)
    with jax.named_scope('gate3'):
        gates(-3)
    with jax.named_scope('hop1half1alse0'):
        hop_on(1, half - 1, False, (0,))
    y_copy(1, lax.rem(s + half - 1, span)).start()
    with jax.named_scope('gate4'):
        gates(4)
    with jax.named_scope('hop1half1alse1'):
        hop_on(1, half - 1, False, (1,))
    y_copy(1, lax.rem(s + half + 1, span)).start()

    @pl.when(s == 0)
    def _():
        edge_zero(0)

    @pl.when(s == span - 1)
    def _():
        edge_zero(EDGE + tokens)

    chip_across = lax.div(across, 2)
    chip_ahead = lax.div(ahead, 2)
    chip_behind = lax.div(behind, 2)
    own_cols = pl.ds(pl.multiple_of(t * cols, cols), cols)

    with jax.named_scope('acti0'):
        activate(0)
    with jax.named_scope('far1b'):
        z_copy(1, 1, far, 1, half).wait_recv()
    y_copy(1, far).start()
    with jax.named_scope('far1a'):
        z_copy(1, 0, far, 0, half).wait_recv()
    with jax.named_scope('giveacross0'):
        give(chip_across, 0)
    with jax.named_scope('acti1'):
        activate(1)
    with jax.named_scope('giveacross1'):
        give(chip_across, 1)
    with jax.named_scope('hop0across0'):
        hop(0, chip_across, 0)
    with jax.named_scope('giveahead0'):
        give(chip_ahead, 0)
    with jax.named_scope('hop0across1'):
        hop(0, chip_across, 1)
    with jax.named_scope('giveahead1'):
        give(chip_ahead, 1)
    with jax.named_scope('hop1behind0'):
        hop(1, chip_behind, 0)
    with jax.named_scope('givebehind0'):
        give(chip_behind, 0)
    with jax.named_scope('hop1behind1'):
        hop(1, chip_behind, 1)
    with jax.named_scope('givebehind1'):
        give(chip_behind, 1)
    with jax.named_scope('keep0'):
        held[0, lots[0]] = joined(chip_ahead, 0)
    with jax.named_scope('give0'):
        give(chip, 0)
    with jax.named_scope('keep1'):
        held[0, lots[1]] = joined(chip_ahead, 1)
    with jax.named_scope('give1'):
        give(chip, 1)
    for h in range(2):
        for q in (2 * h, 2 * h + 1):
            with jax.named_scope('hw0'):
                hop_copy(0, q).wait_recv()
            hop_out[2, parcels[q]] = (held[0, parcels[q]] + hop_in[0, parcels[q]].astype(F32)).astype(BF16)
            hop_copy(2, q).start()
        own_normed = nx_buf[EDGE + h * mid : EDGE + (h + 1) * mid, own_cols].astype(F32)
        held[1, lots[h]] = joined(chip, h) + own_normed
    for q in range(4):
        with jax.named_scope('hw1'):
            hop_copy(1, q).wait_recv()
        with jax.named_scope('hw2'):
            hop_copy(2, q).wait_recv()
        terms = hop_in[1, parcels[q]].astype(F32) + hop_in[2, parcels[q]].astype(F32)
        out_buf[parcels[q], :] = (held[1, parcels[q]] + terms).astype(BF16)
        out_copy(q).start()

    with jax.named_scope('outw'):
        pltpu.make_async_copy(out_buf, out_ref, out_sem).wait()

    def left_all(ref, send, recv):
        remote(ref, ref, send, recv, {"tp": partner}).wait_send()

    left_all(kv_buf.at[0, pl.ds(0, 4 * WINDOW), :], kv_send, kv_recv.at[0, 0])
    left_all(nx_buf.at[pl.ds(0, 2 * EDGE), :], edge_send, edge_recv.at[0, 0])
    left_all(theirs_out, pair_send, pair_recv.at[0, 0])
    left_all(hop_out, hop_send, hop_recv.at[0, 0])
    for way in range(2):
        for kind in range(2):
            for ab in range(2):
                n = half if ab == way else half - 1
                ref = (wide if kind == 0 else tall).at[0, pl.ds(0, n * depth), :]
                row = 2 * kind + ab
                remote(ref, ref, z_send.at[way, row], z_recv.at[way, row, 0], {"sp": right}).wait_send()
    for kind in range(2):
        ref = (wide if kind == 0 else tall).at[0, pl.ds(0, (span - 1) * depth), :]
        remote(ref, ref, y_send.at[kind], y_recv.at[kind, 0], {"grp": pair_grp}).wait_send()
        ref = op_buf.at[pl.ds(0, ranks - 1)] if kind == 0 else mix_buf.at[:, pl.ds(0, (ranks - 1) * HD)]
        remote(ref, ref, x_send.at[kind], x_recv.at[kind, 0], {"tp": partner}).wait_send()


def solution(mesh):
    span, ranks = mesh.shape["sp"], mesh.shape["tp"]

    def shards(q, k, v, sink, resid, out_proj, gain, w_gate, w_up, conv_w, conv_b, w_down):
        tokens, width = resid.shape
        depth, hidden = w_gate.shape
        cols = width // ranks
        chips = ranks // 2
        pw, pd = 2 * hidden // 3, hidden // 3
        there = pl.BlockSpec(memory_space=pltpu.HBM)
        scalar = pl.BlockSpec(memory_space=pltpu.SMEM)
        dma = pltpu.SemaphoreType.DMA
        return pl.pallas_call(
            functools.partial(layer_kernel, span, ranks),
            out_shape=jax.ShapeDtypeStruct((tokens, cols), BF16),
            in_specs=[there, there, there, scalar] + [there] * 8,
            out_specs=there,
            scratch_shapes=[
                pltpu.VMEM((1, width), F32),
                pltpu.VMEM(conv_w.shape, F32),
                pltpu.VMEM(conv_b.shape, F32),
                pltpu.VMEM((tokens, HD), BF16),
                pltpu.VMEM((2, tokens + 2 * WINDOW, HD), BF16),
                pltpu.VMEM((tokens, width), BF16),
                pltpu.VMEM((ranks, out_proj.shape[0], cols), BF16),
                pltpu.VMEM((tokens, ranks * HD), BF16),
                pltpu.VMEM((tokens, width), F32),
                pltpu.VMEM((2, tokens, cols // 2), F32),
                pltpu.VMEM((tokens + 2 * EDGE, width), BF16),
                pltpu.VMEM((3, span * depth, pw), BF16),
                pltpu.VMEM((3, span * depth, pd), BF16),
                pltpu.VMEM((3, tokens + 2 * EDGE, pw), F32),
                pltpu.VMEM((tokens, hidden), BF16),
                pltpu.VMEM((chips, tokens, cols), BF16),
                pltpu.VMEM((chips, tokens, cols), BF16),
                pltpu.VMEM((3, tokens, cols), BF16),
                pltpu.VMEM((3, tokens, cols), BF16),
                pltpu.VMEM((2, tokens, cols), F32),
                pltpu.VMEM((tokens, cols), BF16),
                dma(()),
                dma((9,)),
                dma(()),
                dma((2, 2)),
                dma((2, 4)),
                dma((2, 4, 4)),
                dma((2,)),
                dma((2, ranks)),
                dma((2,)),
                dma((2, ranks)),
                dma(()),
                dma((2, 2)),
                dma(()),
                dma((chips, 2)),
                dma(()),
                dma((3, 4)),
            ],
            compiler_params=pltpu.CompilerParams(
                collective_id=0, has_side_effects=True, vmem_limit_bytes=60 * 1024 * 1024
            ),
        )(
            q, k, v, sink, resid, out_proj, gain.reshape(1, width), w_gate, w_up,
            conv_w, conv_b, w_down.T,
        )

    return jax.shard_map(
        shards,
        mesh=mesh,
        in_specs=(
            P(("grp", "sp"), "tp"),
            P(("grp", "sp"), None),
            P(("grp", "sp"), None),
            P("tp"),
            P(("grp", "sp"), None),
            P(None, "tp"),
            P(),
            P("sp", "tp"),
            P("sp", "tp"),
            P(None, "tp"),
            P("tp"),
            P("tp", "sp"),
        ),
        out_specs=P(("grp", "sp"), "tp"),
        check_vma=False,
    )
```

```python
import functools

import jax
import jax.numpy as jnp
from jax import lax
from jax.experimental import pallas as pl
from jax.experimental.pallas import tpu as pltpu
from jax.sharding import PartitionSpec as P

H = 8
KVH = 2
HD = 128
WINDOW = 128
CONV = 3
EDGE = 16
MESH = pl.DeviceIdType.MESH
F32 = jnp.float32
BF16 = jnp.bfloat16


def layer_kernel(
    span,
    ranks,
    q_hbm,
    k_hbm,
    v_hbm,
    sink_ref,
    res_hbm,
    op_hbm,
    gain_hbm,
    wg_hbm,
    wu_hbm,
    cw_hbm,
    cb_hbm,
    wd_hbm,
    out_ref,
    gain_ref,
    cw_ref,
    cb_ref,
    q_buf,
    kv_buf,
    res_buf,
    op_buf,
    mix_buf,
    summed,
    stat,
    nx_buf,
    wide,
    tall,
    accs,
    act_buf,
    theirs_out,
    theirs_in,
    hop_out,
    hop_in,
    held,
    out_buf,
    out_sem,
    load_sem,
    kv_send,
    kv_recv,
    z_send,
    z_recv,
    y_send,
    y_recv,
    x_send,
    x_recv,
    edge_send,
    edge_recv,
    pair_send,
    pair_recv,
    hop_send,
    hop_recv,
):
    tokens, width = res_buf.shape
    depth, hidden = wg_hbm.shape
    cols = width // ranks
    quad_of = cols // depth
    half = span // 2
    pw = wide.shape[2]
    pd = tall.shape[2]
    chips = ranks // 2

    g = lax.axis_index("grp")
    s = lax.axis_index("sp")
    t = lax.axis_index("tp")
    right, left = lax.rem(s + 1, span), lax.rem(s + span - 1, span)
    parity = lax.rem(g, 2)
    pair_grp = g + 1 - 2 * parity
    own, other = 2 * parity, 2 - 2 * parity
    core = lax.rem(t, 2)
    chip = lax.div(t, 2)
    partner = t + 1 - 2 * core
    ahead = lax.rem(t + 2 - 4 * core + ranks, ranks)
    behind = lax.rem(t - 2 + 4 * core + ranks, ranks)
    across = lax.rem(t + ranks // 2, ranks)
    kv_col = pl.multiple_of(lax.div(t * KVH, ranks) * HD, HD)

    def scoped(name, fn):
        def run():
            with jax.named_scope(name):
                fn()

        return run

    def rows(j):
        return pl.ds(pl.multiple_of(j * depth, depth), depth)

    own_rows = rows(s)
    cut = pw - (hidden - pw)
    def own_copies(sem, pairs):
        return [pltpu.make_async_copy(src, dst, load_sem.at[sem]) for src, dst in pairs]

    def loaded(sem, ref):
        pltpu.make_async_copy(ref, ref, load_sem.at[sem]).wait()

    rest = hidden - pw
    loads = own_copies(
        0,
        [
            (wg_hbm.at[:, pl.ds(0, pw)], wide.at[0, own_rows, :]),
            (wg_hbm.at[:, pl.ds(pw, rest)], wide.at[1, own_rows, pl.ds(0, rest)]),
            (wu_hbm.at[:, pl.ds(0, cut)], wide.at[1, own_rows, pl.ds(rest, cut)]),
            (wu_hbm.at[:, pl.ds(cut, pw)], wide.at[2, own_rows, :]),
        ],
    )
    loads += own_copies(1, [(wd_hbm.at[:, pl.ds(p * pd, pd)], tall.at[p, own_rows, :]) for p in range(3)])
    loads += own_copies(
        2,
        [
            (k_hbm.at[:, pl.ds(kv_col, HD)], kv_buf.at[0, pl.ds(WINDOW, tokens), :]),
            (v_hbm.at[:, pl.ds(kv_col, HD)], kv_buf.at[1, pl.ds(WINDOW, tokens), :]),
        ],
    )
    small = [(q_hbm, q_buf), (op_hbm, op_buf.at[t]), (res_hbm, res_buf), (gain_hbm, gain_ref), (cw_hbm, cw_ref), (cb_hbm, cb_ref)]
    single = [own_copies(3 + i, [pair])[0] for i, pair in enumerate(small)]
    loads += single

    barrier = pltpu.get_barrier_semaphore()
    greeted = ({"sp": right}, {"sp": left}, {"grp": pair_grp}, {"tp": ahead}, {"tp": behind}, {"tp": partner})
    for who in greeted:
        pl.semaphore_signal(barrier, inc=1, device_id=who, device_id_type=MESH)
    for copy in loads:
        copy.start()

    def remote(src, dst, send, recv, who):
        return pltpu.make_async_remote_copy(
            src_ref=src, dst_ref=dst, send_sem=send, recv_sem=recv, device_id=who, device_id_type=MESH
        )

    def part(kind, index, j):
        return (wide if kind == 0 else tall).at[index, rows(j), :]

    def z_copy(kind, ab, j, way, turns):
        ref = part(kind, own if ab else 1, j)
        row = 2 * kind + ab
        recv = z_recv.at[way, row, lax.rem(turns, 4)]
        return remote(ref, ref, z_send.at[way, row], recv, {"sp": left if way else right})

    def y_copy(kind, j):
        ref = part(kind, own, j)
        return remote(ref, ref, y_send.at[kind], y_recv.at[kind, lax.div(j, quad_of)], {"grp": pair_grp})

    def y_arrived(kind, quad):
        def wait(n):
            buf = wide if kind == 0 else tall
            ref = buf.at[other, pl.ds(pl.multiple_of(quad * cols, cols), n * depth), :]
            remote(ref, ref, y_send.at[kind], y_recv.at[kind, quad], {"grp": pair_grp}).wait_recv()

        is_own = quad == lax.div(s, quad_of)

        @pl.when(is_own)
        def _():
            wait(quad_of - 1)

        @pl.when(jnp.logical_not(is_own))
        def _():
            wait(quad_of)

    def block(kind, b):
        if kind == 0:
            return op_buf.at[b]
        return mix_buf.at[:, pl.ds(pl.multiple_of(b * HD, HD), HD)]

    def x_copy(kind, b, slot, who):
        ref = block(kind, b)
        return remote(ref, ref, x_send.at[kind], x_recv.at[kind, b], {"tp": who})

    def x_open(kind):
        x_copy(kind, t, 0, ahead).start()
        x_copy(kind, t, 1, behind).start()
        x_copy(kind, t, 2, partner).start()

    def x_pass(kind):
        x_copy(kind, behind, 3, ahead).wait_recv()
        x_copy(kind, behind, 3, ahead).start()
        x_copy(kind, behind, 4, partner).start()
        x_copy(kind, ahead, 5, partner).wait_recv()
        x_copy(kind, ahead, 5, partner).start()

    def x_last(kind):
        x_copy(kind, across, 6, partner).wait_recv()
        x_copy(kind, across, 6, partner).start()

    def x_close(kind):
        for step in range(chips):
            b = lax.rem(partner + 2 * step, ranks)
            x_copy(kind, b, 0, partner).wait_recv()

    def kv_copy(way):
        here, there = (tokens, 0) if way == 0 else (WINDOW, WINDOW + tokens)
        src, dst = kv_buf.at[core, pl.ds(here, WINDOW), :], kv_buf.at[core, pl.ds(there, WINDOW), :]
        return remote(src, dst, kv_send, kv_recv.at[way, core], {"sp": left if way else right})

    def kv_hand(way, which):
        ref = kv_buf.at[which, pl.ds(WINDOW + tokens if way else 0, WINDOW), :]
        return remote(ref, ref, kv_send, kv_recv.at[way, which], {"tp": partner})

    side = width // 2

    def edge_copy(way):
        here, there = (tokens, 0) if way == 0 else (EDGE, EDGE + tokens)
        lanes = pl.ds(pl.multiple_of(core * side, side), side)
        src, dst = nx_buf.at[pl.ds(here, EDGE), lanes], nx_buf.at[pl.ds(there, EDGE), lanes]
        return remote(src, dst, edge_send, edge_recv.at[way, core], {"sp": left if way else right})

    def edge_hand(way, which):
        lanes = pl.ds(pl.multiple_of(which * side, side), side)
        ref = nx_buf.at[pl.ds(EDGE + tokens if way else 0, EDGE), lanes]
        return remote(ref, ref, edge_send, edge_recv.at[way, which], {"tp": partner})

    def attend(i):
        lo = i * WINDOW
        keys = kv_buf[0, lo : lo + 3 * WINDOW, :]
        vals = kv_buf[1, lo : lo + 3 * WINDOW, :]
        scores = lax.dot_general(
            q_buf[lo : lo + WINDOW, :], keys, (((1,), (1,)), ((), ())), preferred_element_type=F32
        ) * (HD ** (-0.5))
        row = lax.broadcasted_iota(jnp.int32, scores.shape, 0)
        col = lax.broadcasted_iota(jnp.int32, scores.shape, 1)
        pos = s * tokens + (lo - WINDOW) + col
        gap = col - row
        seen = (gap >= 0) & (gap <= 2 * WINDOW) & (pos >= 0) & (pos < span * tokens)
        scores = jnp.where(seen, scores, F32(-1e30))
        sink = sink_ref[0]
        top = jnp.maximum(jnp.max(scores, axis=-1, keepdims=True), sink)
        expo = jnp.exp(scores - top)
        total = jnp.sum(expo, axis=-1, keepdims=True) + jnp.exp(sink - top)
        weights = (expo / total).astype(BF16)
        mixed = jnp.dot(weights, vals, preferred_element_type=F32).astype(BF16)
        mix_buf[lo : lo + WINDOW, pl.ds(pl.multiple_of(t * HD, HD), HD)] = mixed

    def project(o, opens):
        at = pl.ds(pl.multiple_of(o * cols, cols), cols)
        block_sum = res_buf[:, at].astype(F32) + jnp.dot(mix_buf[...], op_buf[o], preferred_element_type=F32)
        summed[:, at] = block_sum
        first, second = block_sum[:, : cols // 2], block_sum[:, cols // 2 :]
        lone = first + second
        squares = first * first + second * second
        if opens:
            stat[0] = lone
            stat[1] = squares
        else:
            stat[0] += lone
            stat[1] += squares

    def normalize(lo, hi):
        @pl.loop(lo // EDGE, hi // EDGE)
        def _(i):
            at = pl.ds(pl.multiple_of(i * EDGE, EDGE), EDGE)
            mean = jnp.sum(stat[0, at, :], axis=-1, keepdims=True) / width
            msq = jnp.sum(stat[1, at, :], axis=-1, keepdims=True) / width
            scale = lax.rsqrt(msq - mean * mean + 1e-05)
            normed = (summed[at, :] - mean) * scale * gain_ref[...]
            nx_buf[pl.ds(pl.multiple_of(i * EDGE + EDGE, EDGE), EDGE), :] = normed.astype(BF16)

    mid = tokens // 2
    lots = [slice(0, mid), slice(mid, tokens)]
    parcels = [slice(q * tokens // 4, (q + 1) * tokens // 4) for q in range(4)]
    quads = span * depth // cols
    mine = lax.div(s * depth, cols)

    def gates(shift, first=False):
        quad = lax.rem(mine + shift + quads, quads)
        at = pl.ds(pl.multiple_of(quad * cols, cols), cols)

        def add(p):
            y = jnp.dot(nx_buf[:, at], wide[p, at, :], preferred_element_type=F32)
            if first:
                accs[p] = y
            else:
                accs[p] += y

        add(1)
        add(own)
        y_arrived(0, quad)
        add(other)

    def edge_zero(where):
        for p in range(2):
            accs[p, where : where + EDGE, :] = jnp.zeros((EDGE, pw), F32)

    def activate(half_of):
        for h in range(3):
            gp, gc = divmod(h * pd, pw)
            up, uc = divmod(hidden + h * pd, pw)
            for r in range(half_of * mid, (half_of + 1) * mid, WINDOW):
                conv = cb_ref[h * pd : (h + 1) * pd].reshape(1, pd)
                for tap in range(CONV):
                    lo = EDGE - CONV // 2 + tap + r
                    gate = accs[gp, lo : lo + WINDOW, gc : gc + pd].astype(BF16).astype(F32)
                    conv = conv + gate * cw_ref[tap : tap + 1, h * pd : (h + 1) * pd]
                ups = accs[up, EDGE + r : EDGE + r + WINDOW, uc : uc + pd].astype(BF16).astype(F32)
                act = conv / (1.0 + jnp.exp(-conv)) * ups
                act_buf[r : r + WINDOW, h * pd : (h + 1) * pd] = act.astype(BF16)

    def partial(o, h):
        lot = lots[h]
        if h == 0:
            y_arrived(1, o)

        at = pl.ds(pl.multiple_of(o * cols, cols), cols)
        total = None
        for p in range(3):
            term = lax.dot_general(
                act_buf[lot, p * pd : (p + 1) * pd],
                tall[p, at, :],
                (((1,), (1,)), ((), ())),
                preferred_element_type=F32,
            )
            total = term if total is None else total + term
        return total

    def pair_copy(owner, h):
        src, dst = theirs_out.at[owner, lots[h]], theirs_in.at[owner, lots[h]]
        return remote(src, dst, pair_send, pair_recv.at[owner, h], {"tp": partner})

    def hop_copy(i, q):
        src, dst = hop_out.at[i, parcels[q]], hop_in.at[i, parcels[q]]
        return remote(src, dst, hop_send, hop_recv.at[i, q], {"tp": behind if i == 1 else ahead})

    def out_copy(q):
        return pltpu.make_async_copy(out_buf.at[parcels[q], :], out_ref.at[parcels[q], :], out_sem)

    def give(owner, h):
        theirs_out[owner, lots[h]] = partial(2 * owner + 1 - core, h).astype(BF16)
        pair_copy(owner, h).start()

    def joined(owner, h):
        kept = partial(2 * owner + core, h)
        pair_copy(owner, h).wait_recv()
        return kept + theirs_in[owner, lots[h]].astype(F32)

    def hop(i, owner, h):
        hop_out[i, lots[h]] = joined(owner, h).astype(BF16)
        hop_copy(i, 2 * h).start()
        hop_copy(i, 2 * h + 1).start()

    blocks = tokens // WINDOW

    def attend_inner():
        for i in range(1, blocks - 1):
            attend(i)

    def unit_attend(inner):
        if inner:
            for way in range(2):
                kv_copy(way).wait_recv()
                kv_hand(way, core).start()
            pl.when(core == 0)(attend_inner)
        else:
            for way in range(2):
                kv_hand(way, 1 - core).wait_recv()
            attend(0)
            attend(blocks - 1)
            x_open(1)

    def unit_edge():
        unit_normalize(2)
        for way in range(2):
            edge_copy(way).wait_recv()
            edge_hand(way, core).start()

    def mirror(b):
        return b + 1 - 2 * lax.rem(b, 2)

    def unit_project(stage):
        if stage == 0:
            x_close(1)
            for copy in single[2:]:
                copy.wait()
            project(t, True)
            project(ahead, False)
        if stage == 1:
            x_last(0)
            x_copy(0, partner, 0, partner).wait_recv()
            project(behind, False)
            project(partner, False)
        if stage == 2:
            for b in (mirror(ahead), mirror(behind)):
                x_copy(0, b, 0, partner).wait_recv()
                project(b, False)
        if stage == 3:
            x_copy(0, mirror(across), 0, partner).wait_recv()
            project(across, False)
            project(mirror(across), False)

    quarter = tokens // 4

    def unit_normalize(i, send=False):
        normalize(i * quarter, (i + 1) * quarter)
        if send:
            for way in range(2):
                edge_copy(way).start()

    def unit_gates(shifts, first=False):
        if first:
            for way in range(2):
                edge_hand(way, 1 - core).wait_recv()
        for i, shift in enumerate(shifts):
            gates(shift, first and i == 0)

    loaded(0, wide.at[:, own_rows, :])
    loaded(1, tall.at[:, own_rows, :])
    loaded(2, kv_buf.at[:, pl.ds(WINDOW, tokens), :])
    single[0].wait()
    with jax.named_scope('bar'):
        pl.semaphore_wait(barrier, len(greeted))

    @pl.when(core == 1)
    def _():
        attend_inner()

    for kind in range(2):
        for turn in range(2):
            for way in range(2):
                z_copy(kind, 1 - turn if kind == 0 or way else turn, s, way, 1).start()
        if kind == 0:
            for way in range(2):
                kv_copy(way).start()
    single[1].wait()
    x_open(0)

    units = {
        (1, 0): lambda: unit_attend(True),
        (1, 1): lambda: unit_attend(False),
        (3, 0): lambda: x_pass(0),
        (3, 1): lambda: x_pass(1),
        (5, 0): lambda: x_last(1),
        (6, 0): lambda: unit_project(0),
        (6, 1): lambda: unit_project(1),
        (7, 0): lambda: unit_project(2),
        (7, 1): lambda: unit_project(3),
        (8, 0): lambda: unit_normalize(0),
        (8, 1): lambda: unit_normalize(3, True),
        (9, 0): lambda: unit_normalize(1),
        (9, 1): unit_edge,
        (10, 0): lambda: unit_gates([0], True),
        (10, 1): lambda: unit_gates([1]),
        (11, 0): lambda: unit_gates([-1]),
        (12, 1): lambda: unit_gates([2]),
        (13, 0): lambda: unit_gates([-2]),
    }

    def hop_part(kind, ab, way, k, swap):
        j = lax.rem(s + k, span) if way else lax.rem(s - k + span, span)
        z_copy(kind, ab, j, way, k).wait_recv()
        if ab == way:
            z_copy(kind, ab, j, way, k + 1).start()
        else:

            @pl.when(k < half - 1)
            def _():
                z_copy(kind, ab, j, way, k + 1).start()

        if ab == 1 and swap is not False:
            pl.when(swap)(y_copy(kind, j).start)

    def hop_down(k, swap, turns):
        for turn in turns:
            for way in range(2):
                hop_part(1, turn if way == 0 else 1 - turn, way, k, swap)

    def swap_down(k):
        y_copy(1, lax.rem(s - k + span, span)).start()
        y_copy(1, lax.rem(s + k, span)).start()

    def ring_wide(ab, k):
        for way in range(2):
            hop_part(0, ab, way, k, True)

    def ring_tall(k):
        hop_down(k - 1, k < half - 1, (0, 1))

    @pl.loop(1, half)
    def _(k):
        with jax.named_scope('hopb'):
            ring_wide(1, k)

        @pl.when(k > 1)
        def _():
            with jax.named_scope('hopa'):
                ring_wide(0, k - 1)

        for (step, slot), unit in units.items():
            if slot == 0:
                pl.when(k == step)(unit)

        @pl.when(k > 1)
        def _():
            with jax.named_scope('hopd'):
                ring_tall(k)

        for (step, slot), unit in units.items():
            if slot == 1:
                pl.when(k == step)(unit)

    far = lax.rem(s + half, span)
    with jax.named_scope('far0b'):
        z_copy(0, 1, far, 1, half).wait_recv()
    y_copy(0, far).start()
    swap_down(half - 2)
    with jax.named_scope('ring0half1'):
        ring_wide(0, half - 1)
    with jax.named_scope('gate3'):
        gates(3)
    with jax.named_scope('gate3'):
        gates(-3)
    with jax.named_scope('hophalf1alse0'):
        hop_down(half - 1, False, (0,))
    y_copy(1, lax.rem(s + half - 1, span)).start()
    with jax.named_scope('far0a'):
        z_copy(0, 0, far, 0, half).wait_recv()
    with jax.named_scope('gate4'):
        gates(4)
    with jax.named_scope('hophalf1alse1'):
        hop_down(half - 1, False, (1,))
    y_copy(1, lax.rem(s + half + 1, span)).start()

    @pl.when(s == 0)
    def _():
        edge_zero(0)

    @pl.when(s == span - 1)
    def _():
        edge_zero(EDGE + tokens)

    chip_across = lax.div(across, 2)
    chip_ahead = lax.div(ahead, 2)
    chip_behind = lax.div(behind, 2)
    own_cols = pl.ds(pl.multiple_of(t * cols, cols), cols)

    with jax.named_scope('acti0'):
        activate(0)
    with jax.named_scope('far1b'):
        z_copy(1, 1, far, 1, half).wait_recv()
    y_copy(1, far).start()
    with jax.named_scope('far1a'):
        z_copy(1, 0, far, 0, half).wait_recv()
    with jax.named_scope('giveacross0'):
        give(chip_across, 0)
    with jax.named_scope('acti1'):
        activate(1)
    with jax.named_scope('giveacross1'):
        give(chip_across, 1)
    with jax.named_scope('hop0across0'):
        hop(0, chip_across, 0)
    with jax.named_scope('giveahead0'):
        give(chip_ahead, 0)
    with jax.named_scope('hop0across1'):
        hop(0, chip_across, 1)
    with jax.named_scope('giveahead1'):
        give(chip_ahead, 1)
    with jax.named_scope('hop1behind0'):
        hop(1, chip_behind, 0)
    with jax.named_scope('givebehind0'):
        give(chip_behind, 0)
    with jax.named_scope('hop1behind1'):
        hop(1, chip_behind, 1)
    with jax.named_scope('givebehind1'):
        give(chip_behind, 1)
    with jax.named_scope('keep0'):
        held[0, lots[0]] = joined(chip_ahead, 0)
    with jax.named_scope('give0'):
        give(chip, 0)
    with jax.named_scope('keep1'):
        held[0, lots[1]] = joined(chip_ahead, 1)
    with jax.named_scope('give1'):
        give(chip, 1)
    for h in range(2):
        for q in (2 * h, 2 * h + 1):
            with jax.named_scope('hw0'):
                hop_copy(0, q).wait_recv()
            hop_out[2, parcels[q]] = (held[0, parcels[q]] + hop_in[0, parcels[q]].astype(F32)).astype(BF16)
            hop_copy(2, q).start()
        own_normed = nx_buf[EDGE + h * mid : EDGE + (h + 1) * mid, own_cols].astype(F32)
        held[1, lots[h]] = joined(chip, h) + own_normed
    for q in range(4):
        with jax.named_scope('hw1'):
            hop_copy(1, q).wait_recv()
        with jax.named_scope('hw2'):
            hop_copy(2, q).wait_recv()
        terms = hop_in[1, parcels[q]].astype(F32) + hop_in[2, parcels[q]].astype(F32)
        out_buf[parcels[q], :] = (held[1, parcels[q]] + terms).astype(BF16)
        out_copy(q).start()

    with jax.named_scope('outw'):
        pltpu.make_async_copy(out_buf, out_ref, out_sem).wait()

    def left_all(ref, send, recv):
        remote(ref, ref, send, recv, {"tp": partner}).wait_send()

    left_all(kv_buf.at[0, pl.ds(0, 4 * WINDOW), :], kv_send, kv_recv.at[0, 0])
    left_all(nx_buf.at[pl.ds(0, 2 * EDGE), :], edge_send, edge_recv.at[0, 0])
    left_all(theirs_out, pair_send, pair_recv.at[0, 0])
    left_all(hop_out, hop_send, hop_recv.at[0, 0])
    for way in range(2):
        for kind in range(2):
            for ab in range(2):
                n = half if ab == way else half - 1
                ref = (wide if kind == 0 else tall).at[0, pl.ds(0, n * depth), :]
                row = 2 * kind + ab
                remote(ref, ref, z_send.at[way, row], z_recv.at[way, row, 0], {"sp": right}).wait_send()
    for kind in range(2):
        ref = (wide if kind == 0 else tall).at[0, pl.ds(0, (span - 1) * depth), :]
        remote(ref, ref, y_send.at[kind], y_recv.at[kind, 0], {"grp": pair_grp}).wait_send()
        ref = op_buf.at[pl.ds(0, ranks - 1)] if kind == 0 else mix_buf.at[:, pl.ds(0, (ranks - 1) * HD)]
        remote(ref, ref, x_send.at[kind], x_recv.at[kind, 0], {"tp": partner}).wait_send()


def solution(mesh):
    span, ranks = mesh.shape["sp"], mesh.shape["tp"]

    def shards(q, k, v, sink, resid, out_proj, gain, w_gate, w_up, conv_w, conv_b, w_down):
        tokens, width = resid.shape
        depth, hidden = w_gate.shape
        cols = width // ranks
        chips = ranks // 2
        pw, pd = 2 * hidden // 3, hidden // 3
        there = pl.BlockSpec(memory_space=pltpu.HBM)
        scalar = pl.BlockSpec(memory_space=pltpu.SMEM)
        dma = pltpu.SemaphoreType.DMA
        return pl.pallas_call(
            functools.partial(layer_kernel, span, ranks),
            out_shape=jax.ShapeDtypeStruct((tokens, cols), BF16),
            in_specs=[there, there, there, scalar] + [there] * 8,
            out_specs=there,
            scratch_shapes=[
                pltpu.VMEM((1, width), F32),
                pltpu.VMEM(conv_w.shape, F32),
                pltpu.VMEM(conv_b.shape, F32),
                pltpu.VMEM((tokens, HD), BF16),
                pltpu.VMEM((2, tokens + 2 * WINDOW, HD), BF16),
                pltpu.VMEM((tokens, width), BF16),
                pltpu.VMEM((ranks, out_proj.shape[0], cols), BF16),
                pltpu.VMEM((tokens, ranks * HD), BF16),
                pltpu.VMEM((tokens, width), F32),
                pltpu.VMEM((2, tokens, cols // 2), F32),
                pltpu.VMEM((tokens + 2 * EDGE, width), BF16),
                pltpu.VMEM((3, span * depth, pw), BF16),
                pltpu.VMEM((3, span * depth, pd), BF16),
                pltpu.VMEM((3, tokens + 2 * EDGE, pw), F32),
                pltpu.VMEM((tokens, hidden), BF16),
                pltpu.VMEM((chips, tokens, cols), BF16),
                pltpu.VMEM((chips, tokens, cols), BF16),
                pltpu.VMEM((3, tokens, cols), BF16),
                pltpu.VMEM((3, tokens, cols), BF16),
                pltpu.VMEM((2, tokens, cols), F32),
                pltpu.VMEM((tokens, cols), BF16),
                dma(()),
                dma((9,)),
                dma(()),
                dma((2, 2)),
                dma((2, 4)),
                dma((2, 4, 4)),
                dma((2,)),
                dma((2, ranks)),
                dma((2,)),
                dma((2, ranks)),
                dma(()),
                dma((2, 2)),
                dma(()),
                dma((chips, 2)),
                dma(()),
                dma((3, 4)),
            ],
            compiler_params=pltpu.CompilerParams(
                collective_id=0, has_side_effects=True, vmem_limit_bytes=60 * 1024 * 1024
            ),
        )(
            q, k, v, sink, resid, out_proj, gain.reshape(1, width), w_gate, w_up,
            conv_w, conv_b, w_down.T,
        )

    return jax.shard_map(
        shards,
        mesh=mesh,
        in_specs=(
            P(("grp", "sp"), "tp"),
            P(("grp", "sp"), None),
            P(("grp", "sp"), None),
            P("tp"),
            P(("grp", "sp"), None),
            P(None, "tp"),
            P(),
            P("sp", "tp"),
            P("sp", "tp"),
            P(None, "tp"),
            P("tp"),
            P("tp", "sp"),
        ),
        out_specs=P(("grp", "sp"), "tp"),
        check_vma=False,
    )
```

```python
import functools

import jax
import jax.numpy as jnp
from jax import lax
from jax.experimental import pallas as pl
from jax.experimental.pallas import tpu as pltpu
from jax.sharding import PartitionSpec as P

H = 8
KVH = 2
HD = 128
WINDOW = 128
CONV = 3
EDGE = 16
MESH = pl.DeviceIdType.MESH
F32 = jnp.float32
BF16 = jnp.bfloat16


def layer_kernel(
    span,
    ranks,
    q_hbm,
    k_hbm,
    v_hbm,
    sink_ref,
    res_hbm,
    op_hbm,
    gain_hbm,
    wg_hbm,
    wu_hbm,
    cw_hbm,
    cb_hbm,
    wd_hbm,
    out_ref,
    gain_ref,
    cw_ref,
    cb_ref,
    q_buf,
    kv_buf,
    res_buf,
    op_buf,
    mix_buf,
    summed,
    stat,
    nx_buf,
    wide,
    tall,
    accs,
    act_buf,
    theirs_out,
    theirs_in,
    hop_out,
    hop_in,
    held,
    out_buf,
    out_sem,
    load_sem,
    kv_send,
    kv_recv,
    z_send,
    z_recv,
    y_send,
    y_recv,
    x_send,
    x_recv,
    edge_send,
    edge_recv,
    pair_send,
    pair_recv,
    hop_send,
    hop_recv,
):
    tokens, width = res_buf.shape
    depth, hidden = wg_hbm.shape
    cols = width // ranks
    quad_of = cols // depth
    half = span // 2
    pw = wide.shape[2]
    pd = tall.shape[2]
    chips = ranks // 2

    g = lax.axis_index("grp")
    s = lax.axis_index("sp")
    t = lax.axis_index("tp")
    right, left = lax.rem(s + 1, span), lax.rem(s + span - 1, span)
    parity = lax.rem(g, 2)
    pair_grp = g + 1 - 2 * parity
    own, other = 2 * parity, 2 - 2 * parity
    core = lax.rem(t, 2)
    chip = lax.div(t, 2)
    partner = t + 1 - 2 * core
    ahead = lax.rem(t + 2 - 4 * core + ranks, ranks)
    behind = lax.rem(t - 2 + 4 * core + ranks, ranks)
    across = lax.rem(t + ranks // 2, ranks)
    kv_col = pl.multiple_of(lax.div(t * KVH, ranks) * HD, HD)

    def rows(j):
        return pl.ds(pl.multiple_of(j * depth, depth), depth)

    own_rows = rows(s)
    cut = pw - (hidden - pw)
    def own_copies(sem, pairs):
        return [pltpu.make_async_copy(src, dst, load_sem.at[sem]) for src, dst in pairs]

    def loaded(sem, ref):
        pltpu.make_async_copy(ref, ref, load_sem.at[sem]).wait()

    rest = hidden - pw
    loads = own_copies(
        0,
        [
            (wg_hbm.at[:, pl.ds(0, pw)], wide.at[0, own_rows, :]),
            (wg_hbm.at[:, pl.ds(pw, rest)], wide.at[1, own_rows, pl.ds(0, rest)]),
            (wu_hbm.at[:, pl.ds(0, cut)], wide.at[1, own_rows, pl.ds(rest, cut)]),
            (wu_hbm.at[:, pl.ds(cut, pw)], wide.at[2, own_rows, :]),
        ],
    )
    loads += own_copies(1, [(wd_hbm.at[:, pl.ds(p * pd, pd)], tall.at[p, own_rows, :]) for p in range(3)])
    loads += own_copies(
        2,
        [
            (k_hbm.at[:, pl.ds(kv_col, HD)], kv_buf.at[0, pl.ds(WINDOW, tokens), :]),
            (v_hbm.at[:, pl.ds(kv_col, HD)], kv_buf.at[1, pl.ds(WINDOW, tokens), :]),
        ],
    )
    small = [(q_hbm, q_buf), (op_hbm, op_buf.at[t]), (res_hbm, res_buf), (gain_hbm, gain_ref), (cw_hbm, cw_ref), (cb_hbm, cb_ref)]
    single = [own_copies(3 + i, [pair])[0] for i, pair in enumerate(small)]
    loads += single

    barrier = pltpu.get_barrier_semaphore()
    greeted = ({"sp": right}, {"sp": left}, {"grp": pair_grp}, {"tp": ahead}, {"tp": behind}, {"tp": partner})
    for who in greeted:
        pl.semaphore_signal(barrier, inc=1, device_id=who, device_id_type=MESH)
    for copy in loads:
        copy.start()

    def remote(src, dst, send, recv, who):
        return pltpu.make_async_remote_copy(
            src_ref=src, dst_ref=dst, send_sem=send, recv_sem=recv, device_id=who, device_id_type=MESH
        )

    def part(kind, index, j):
        return (wide if kind == 0 else tall).at[index, rows(j), :]

    def z_copy(kind, ab, j, way, turns):
        ref = part(kind, own if ab else 1, j)
        row = 2 * kind + ab
        recv = z_recv.at[way, row, lax.rem(turns, 4)]
        return remote(ref, ref, z_send.at[way, row], recv, {"sp": left if way else right})

    def y_copy(kind, j):
        ref = part(kind, own, j)
        return remote(ref, ref, y_send.at[kind], y_recv.at[kind, lax.div(j, quad_of)], {"grp": pair_grp})

    def y_arrived(kind, quad):
        def wait(n):
            buf = wide if kind == 0 else tall
            ref = buf.at[other, pl.ds(pl.multiple_of(quad * cols, cols), n * depth), :]
            remote(ref, ref, y_send.at[kind], y_recv.at[kind, quad], {"grp": pair_grp}).wait_recv()

        is_own = quad == lax.div(s, quad_of)

        @pl.when(is_own)
        def _():
            wait(quad_of - 1)

        @pl.when(jnp.logical_not(is_own))
        def _():
            wait(quad_of)

    def block(kind, b):
        if kind == 0:
            return op_buf.at[b]
        return mix_buf.at[:, pl.ds(pl.multiple_of(b * HD, HD), HD)]

    def x_copy(kind, b, slot, who):
        ref = block(kind, b)
        return remote(ref, ref, x_send.at[kind], x_recv.at[kind, b], {"tp": who})

    def x_open(kind):
        x_copy(kind, t, 0, ahead).start()
        x_copy(kind, t, 1, behind).start()
        x_copy(kind, t, 2, partner).start()

    def x_pass(kind):
        x_copy(kind, behind, 3, ahead).wait_recv()
        x_copy(kind, behind, 3, ahead).start()
        x_copy(kind, behind, 4, partner).start()
        x_copy(kind, ahead, 5, partner).wait_recv()
        x_copy(kind, ahead, 5, partner).start()

    def x_last(kind):
        x_copy(kind, across, 6, partner).wait_recv()
        x_copy(kind, across, 6, partner).start()

    def x_close(kind):
        for step in range(chips):
            b = lax.rem(partner + 2 * step, ranks)
            x_copy(kind, b, 0, partner).wait_recv()

    def kv_copy(way):
        here, there = (tokens, 0) if way == 0 else (WINDOW, WINDOW + tokens)
        src, dst = kv_buf.at[core, pl.ds(here, WINDOW), :], kv_buf.at[core, pl.ds(there, WINDOW), :]
        return remote(src, dst, kv_send, kv_recv.at[way, core], {"sp": left if way else right})

    def kv_hand(way, which):
        ref = kv_buf.at[which, pl.ds(WINDOW + tokens if way else 0, WINDOW), :]
        return remote(ref, ref, kv_send, kv_recv.at[way, which], {"tp": partner})

    side = width // 2

    def edge_copy(way):
        here, there = (tokens, 0) if way == 0 else (EDGE, EDGE + tokens)
        lanes = pl.ds(pl.multiple_of(core * side, side), side)
        src, dst = nx_buf.at[pl.ds(here, EDGE), lanes], nx_buf.at[pl.ds(there, EDGE), lanes]
        return remote(src, dst, edge_send, edge_recv.at[way, core], {"sp": left if way else right})

    def edge_hand(way, which):
        lanes = pl.ds(pl.multiple_of(which * side, side), side)
        ref = nx_buf.at[pl.ds(EDGE + tokens if way else 0, EDGE), lanes]
        return remote(ref, ref, edge_send, edge_recv.at[way, which], {"tp": partner})

    def attend(i):
        lo = i * WINDOW
        keys = kv_buf[0, lo : lo + 3 * WINDOW, :]
        vals = kv_buf[1, lo : lo + 3 * WINDOW, :]
        scores = lax.dot_general(
            q_buf[lo : lo + WINDOW, :], keys, (((1,), (1,)), ((), ())), preferred_element_type=F32
        ) * (HD ** (-0.5))
        row = lax.broadcasted_iota(jnp.int32, scores.shape, 0)
        col = lax.broadcasted_iota(jnp.int32, scores.shape, 1)
        pos = s * tokens + (lo - WINDOW) + col
        gap = col - row
        seen = (gap >= 0) & (gap <= 2 * WINDOW) & (pos >= 0) & (pos < span * tokens)
        scores = jnp.where(seen, scores, F32(-1e30))
        sink = sink_ref[0]
        top = jnp.maximum(jnp.max(scores, axis=-1, keepdims=True), sink)
        expo = jnp.exp(scores - top)
        total = jnp.sum(expo, axis=-1, keepdims=True) + jnp.exp(sink - top)
        weights = (expo / total).astype(BF16)
        mixed = jnp.dot(weights, vals, preferred_element_type=F32).astype(BF16)
        mix_buf[lo : lo + WINDOW, pl.ds(pl.multiple_of(t * HD, HD), HD)] = mixed

    def project(o, opens):
        at = pl.ds(pl.multiple_of(o * cols, cols), cols)
        block_sum = res_buf[:, at].astype(F32) + jnp.dot(mix_buf[...], op_buf[o], preferred_element_type=F32)
        summed[:, at] = block_sum
        first, second = block_sum[:, : cols // 2], block_sum[:, cols // 2 :]
        lone = first + second
        squares = first * first + second * second
        if opens:
            stat[0] = lone
            stat[1] = squares
        else:
            stat[0] += lone
            stat[1] += squares

    def normalize(lo, hi):
        @pl.loop(lo // EDGE, hi // EDGE)
        def _(i):
            at = pl.ds(pl.multiple_of(i * EDGE, EDGE), EDGE)
            mean = jnp.sum(stat[0, at, :], axis=-1, keepdims=True) / width
            msq = jnp.sum(stat[1, at, :], axis=-1, keepdims=True) / width
            scale = lax.rsqrt(msq - mean * mean + 1e-05)
            normed = (summed[at, :] - mean) * scale * gain_ref[...]
            nx_buf[pl.ds(pl.multiple_of(i * EDGE + EDGE, EDGE), EDGE), :] = normed.astype(BF16)

    mid = tokens // 2
    lots = [slice(0, mid), slice(mid, tokens)]
    parcels = [slice(q * tokens // 4, (q + 1) * tokens // 4) for q in range(4)]
    quads = span * depth // cols
    mine = lax.div(s * depth, cols)

    def gates(shift, first=False):
        quad = lax.rem(mine + shift + quads, quads)
        at = pl.ds(pl.multiple_of(quad * cols, cols), cols)

        def add(p):
            y = jnp.dot(nx_buf[:, at], wide[p, at, :], preferred_element_type=F32)
            if first:
                accs[p] = y
            else:
                accs[p] += y

        add(1)
        add(own)
        y_arrived(0, quad)
        add(other)

    def edge_zero(where):
        for p in range(2):
            accs[p, where : where + EDGE, :] = jnp.zeros((EDGE, pw), F32)

    def activate(half_of):
        for h in range(3):
            gp, gc = divmod(h * pd, pw)
            up, uc = divmod(hidden + h * pd, pw)
            for r in range(half_of * mid, (half_of + 1) * mid, WINDOW):
                conv = cb_ref[h * pd : (h + 1) * pd].reshape(1, pd)
                for tap in range(CONV):
                    lo = EDGE - CONV // 2 + tap + r
                    gate = accs[gp, lo : lo + WINDOW, gc : gc + pd].astype(BF16).astype(F32)
                    conv = conv + gate * cw_ref[tap : tap + 1, h * pd : (h + 1) * pd]
                ups = accs[up, EDGE + r : EDGE + r + WINDOW, uc : uc + pd].astype(BF16).astype(F32)
                act = conv / (1.0 + jnp.exp(-conv)) * ups
                act_buf[r : r + WINDOW, h * pd : (h + 1) * pd] = act.astype(BF16)

    def partial(o, h):
        lot = lots[h]
        if h == 0:
            y_arrived(1, o)

        at = pl.ds(pl.multiple_of(o * cols, cols), cols)
        total = None
        for p in range(3):
            term = lax.dot_general(
                act_buf[lot, p * pd : (p + 1) * pd],
                tall[p, at, :],
                (((1,), (1,)), ((), ())),
                preferred_element_type=F32,
            )
            total = term if total is None else total + term
        return total

    def pair_copy(owner, h):
        src, dst = theirs_out.at[owner, lots[h]], theirs_in.at[owner, lots[h]]
        return remote(src, dst, pair_send, pair_recv.at[owner, h], {"tp": partner})

    def hop_copy(i, q):
        src, dst = hop_out.at[i, parcels[q]], hop_in.at[i, parcels[q]]
        return remote(src, dst, hop_send, hop_recv.at[i, q], {"tp": behind if i == 1 else ahead})

    def out_copy(q):
        return pltpu.make_async_copy(out_buf.at[parcels[q], :], out_ref.at[parcels[q], :], out_sem)

    def give(owner, h):
        theirs_out[owner, lots[h]] = partial(2 * owner + 1 - core, h).astype(BF16)
        pair_copy(owner, h).start()

    def joined(owner, h):
        kept = partial(2 * owner + core, h)
        pair_copy(owner, h).wait_recv()
        return kept + theirs_in[owner, lots[h]].astype(F32)

    def hop(i, owner, h):
        hop_out[i, lots[h]] = joined(owner, h).astype(BF16)
        hop_copy(i, 2 * h).start()
        hop_copy(i, 2 * h + 1).start()

    blocks = tokens // WINDOW

    def attend_inner():
        for i in range(1, blocks - 1):
            attend(i)

    def unit_attend(inner):
        if inner:
            for way in range(2):
                kv_copy(way).wait_recv()
                kv_hand(way, core).start()
            pl.when(core == 0)(attend_inner)
        else:
            for way in range(2):
                kv_hand(way, 1 - core).wait_recv()
            attend(0)
            attend(blocks - 1)
            x_open(1)

    def unit_edge():
        for way in range(2):
            edge_copy(way).wait_recv()
            edge_hand(way, core).start()

    def mirror(b):
        return b + 1 - 2 * lax.rem(b, 2)

    def unit_project(stage):
        if stage == 0:
            x_close(1)
            for copy in single[2:]:
                copy.wait()
            project(t, True)
            project(ahead, False)
        if stage == 1:
            x_last(0)
            x_copy(0, partner, 0, partner).wait_recv()
            project(behind, False)
            project(partner, False)
        if stage == 2:
            for b in (mirror(ahead), mirror(behind)):
                x_copy(0, b, 0, partner).wait_recv()
                project(b, False)
        if stage == 3:
            x_copy(0, mirror(across), 0, partner).wait_recv()
            project(across, False)
            project(mirror(across), False)

    quarter = tokens // 4

    def unit_normalize(i, send=False):
        normalize(i * quarter, (i + 1) * quarter)
        if send:
            for way in range(2):
                edge_copy(way).start()

    def unit_gates(shifts, first=False):
        if first:
            for way in range(2):
                edge_hand(way, 1 - core).wait_recv()
        for i, shift in enumerate(shifts):
            gates(shift, first and i == 0)

    loaded(0, wide.at[:, own_rows, :])
    loaded(1, tall.at[:, own_rows, :])
    loaded(2, kv_buf.at[:, pl.ds(WINDOW, tokens), :])
    single[0].wait()
    pl.semaphore_wait(barrier, len(greeted))

    @pl.when(core == 1)
    def _():
        attend_inner()

    for kind in range(2):
        for turn in range(2):
            for way in range(2):
                z_copy(kind, turn if way == 0 else 1 - turn, s, way, 1).start()
        if kind == 0:
            for way in range(2):
                kv_copy(way).start()
    single[1].wait()
    x_open(0)

    units = {
        (1, 0): lambda: unit_attend(True),
        (1, 1): lambda: unit_attend(False),
        (3, 0): lambda: x_pass(0),
        (3, 1): lambda: x_pass(1),
        (6, 0): lambda: x_last(1),
        (6, 1): lambda: unit_project(0),
        (7, 0): lambda: unit_project(1),
        (7, 1): lambda: unit_project(2),
        (8, 0): lambda: unit_project(3),
        (8, 1): lambda: unit_normalize(0),
        (9, 0): lambda: unit_normalize(3, True),
        (9, 1): lambda: unit_normalize(1),
        (10, 0): lambda: unit_normalize(2),
        (10, 1): unit_edge,
        (11, 1): lambda: unit_gates([0], True),
        (12, 0): lambda: unit_gates([1]),
        (12, 1): lambda: unit_gates([-1]),
        (13, 0): lambda: unit_gates([2]),
        (13, 1): lambda: unit_gates([-2]),
    }

    def hop_on(kind, k, swap, turns=(0, 1)):
        back = lax.rem(s - k + span, span)
        front = lax.rem(s + k, span)
        for turn in turns:
            for way, j in ((0, back), (1, front)):
                ab = turn if way == 0 else 1 - turn
                z_copy(kind, ab, j, way, k).wait_recv()
                if ab == way:
                    z_copy(kind, ab, j, way, k + 1).start()
                else:

                    @pl.when(k < half - 1)
                    def _():
                        z_copy(kind, ab, j, way, k + 1).start()

                if ab == 1 and swap is not False:
                    pl.when(swap)(y_copy(kind, j).start)

    def swap_down(k):
        y_copy(1, lax.rem(s - k + span, span)).start()
        y_copy(1, lax.rem(s + k, span)).start()

    def ring_wide(k):
        hop_on(0, k, True)

    def ring_tall(k):
        hop_on(1, k, k < half - 1)

    @pl.loop(1, half)
    def _(k):
        ring_wide(k)
        for (step, slot), unit in units.items():
            if slot == 0:
                pl.when(k == step)(unit)

        ring_tall(k)
        for (step, slot), unit in units.items():
            if slot == 1:
                pl.when(k == step)(unit)

    far = lax.rem(s + half, span)
    z_copy(0, 1, far, 1, half).wait_recv()
    y_copy(0, far).start()
    swap_down(half - 1)
    z_copy(0, 0, far, 0, half).wait_recv()

    gates(3)
    gates(-3)
    gates(4)

    @pl.when(s == 0)
    def _():
        edge_zero(0)

    @pl.when(s == span - 1)
    def _():
        edge_zero(EDGE + tokens)

    chip_across = lax.div(across, 2)
    chip_ahead = lax.div(ahead, 2)
    chip_behind = lax.div(behind, 2)
    own_cols = pl.ds(pl.multiple_of(t * cols, cols), cols)

    activate(0)
    z_copy(1, 1, far, 1, half).wait_recv()
    y_copy(1, far).start()
    z_copy(1, 0, far, 0, half).wait_recv()
    give(chip_across, 0)
    activate(1)
    give(chip_across, 1)
    hop(0, chip_across, 0)
    give(chip_ahead, 0)
    hop(0, chip_across, 1)
    give(chip_ahead, 1)
    hop(1, chip_behind, 0)
    give(chip_behind, 0)
    hop(1, chip_behind, 1)
    give(chip_behind, 1)
    held[0, lots[0]] = joined(chip_ahead, 0)
    give(chip, 0)
    held[0, lots[1]] = joined(chip_ahead, 1)
    give(chip, 1)
    for h in range(2):
        for q in (2 * h, 2 * h + 1):
            hop_copy(0, q).wait_recv()
            hop_out[2, parcels[q]] = (held[0, parcels[q]] + hop_in[0, parcels[q]].astype(F32)).astype(BF16)
            hop_copy(2, q).start()
        own_normed = nx_buf[EDGE + h * mid : EDGE + (h + 1) * mid, own_cols].astype(F32)
        held[1, lots[h]] = joined(chip, h) + own_normed
    for q in range(4):
        hop_copy(1, q).wait_recv()
        hop_copy(2, q).wait_recv()
        terms = hop_in[1, parcels[q]].astype(F32) + hop_in[2, parcels[q]].astype(F32)
        out_buf[parcels[q], :] = (held[1, parcels[q]] + terms).astype(BF16)
        out_copy(q).start()

    pltpu.make_async_copy(out_buf, out_ref, out_sem).wait()

    def left_all(ref, send, recv):
        remote(ref, ref, send, recv, {"tp": partner}).wait_send()

    left_all(kv_buf.at[0, pl.ds(0, 4 * WINDOW), :], kv_send, kv_recv.at[0, 0])
    left_all(nx_buf.at[pl.ds(0, 2 * EDGE), :], edge_send, edge_recv.at[0, 0])
    left_all(theirs_out, pair_send, pair_recv.at[0, 0])
    left_all(hop_out, hop_send, hop_recv.at[0, 0])
    for way in range(2):
        for kind in range(2):
            for ab in range(2):
                n = half if ab == way else half - 1
                ref = (wide if kind == 0 else tall).at[0, pl.ds(0, n * depth), :]
                row = 2 * kind + ab
                remote(ref, ref, z_send.at[way, row], z_recv.at[way, row, 0], {"sp": right}).wait_send()
    for kind in range(2):
        ref = (wide if kind == 0 else tall).at[0, pl.ds(0, (span - 1) * depth), :]
        remote(ref, ref, y_send.at[kind], y_recv.at[kind, 0], {"grp": pair_grp}).wait_send()
        ref = op_buf.at[pl.ds(0, ranks - 1)] if kind == 0 else mix_buf.at[:, pl.ds(0, (ranks - 1) * HD)]
        remote(ref, ref, x_send.at[kind], x_recv.at[kind, 0], {"tp": partner}).wait_send()


def solution(mesh):
    span, ranks = mesh.shape["sp"], mesh.shape["tp"]

    def shards(q, k, v, sink, resid, out_proj, gain, w_gate, w_up, conv_w, conv_b, w_down):
        tokens, width = resid.shape
        depth, hidden = w_gate.shape
        cols = width // ranks
        chips = ranks // 2
        pw, pd = 2 * hidden // 3, hidden // 3
        there = pl.BlockSpec(memory_space=pltpu.HBM)
        scalar = pl.BlockSpec(memory_space=pltpu.SMEM)
        dma = pltpu.SemaphoreType.DMA
        return pl.pallas_call(
            functools.partial(layer_kernel, span, ranks),
            out_shape=jax.ShapeDtypeStruct((tokens, cols), BF16),
            in_specs=[there, there, there, scalar] + [there] * 8,
            out_specs=there,
            scratch_shapes=[
                pltpu.VMEM((1, width), F32),
                pltpu.VMEM(conv_w.shape, F32),
                pltpu.VMEM(conv_b.shape, F32),
                pltpu.VMEM((tokens, HD), BF16),
                pltpu.VMEM((2, tokens + 2 * WINDOW, HD), BF16),
                pltpu.VMEM((tokens, width), BF16),
                pltpu.VMEM((ranks, out_proj.shape[0], cols), BF16),
                pltpu.VMEM((tokens, ranks * HD), BF16),
                pltpu.VMEM((tokens, width), F32),
                pltpu.VMEM((2, tokens, cols // 2), F32),
                pltpu.VMEM((tokens + 2 * EDGE, width), BF16),
                pltpu.VMEM((3, span * depth, pw), BF16),
                pltpu.VMEM((3, span * depth, pd), BF16),
                pltpu.VMEM((3, tokens + 2 * EDGE, pw), F32),
                pltpu.VMEM((tokens, hidden), BF16),
                pltpu.VMEM((chips, tokens, cols), BF16),
                pltpu.VMEM((chips, tokens, cols), BF16),
                pltpu.VMEM((3, tokens, cols), BF16),
                pltpu.VMEM((3, tokens, cols), BF16),
                pltpu.VMEM((2, tokens, cols), F32),
                pltpu.VMEM((tokens, cols), BF16),
                dma(()),
                dma((9,)),
                dma(()),
                dma((2, 2)),
                dma((2, 4)),
                dma((2, 4, 4)),
                dma((2,)),
                dma((2, ranks)),
                dma((2,)),
                dma((2, ranks)),
                dma(()),
                dma((2, 2)),
                dma(()),
                dma((chips, 2)),
                dma(()),
                dma((3, 4)),
            ],
            compiler_params=pltpu.CompilerParams(
                collective_id=0, has_side_effects=True, vmem_limit_bytes=60 * 1024 * 1024
            ),
        )(
            q, k, v, sink, resid, out_proj, gain.reshape(1, width), w_gate, w_up,
            conv_w, conv_b, w_down.T,
        )

    return jax.shard_map(
        shards,
        mesh=mesh,
        in_specs=(
            P(("grp", "sp"), "tp"),
            P(("grp", "sp"), None),
            P(("grp", "sp"), None),
            P("tp"),
            P(("grp", "sp"), None),
            P(None, "tp"),
            P(),
            P("sp", "tp"),
            P("sp", "tp"),
            P(None, "tp"),
            P("tp"),
            P("tp", "sp"),
        ),
        out_specs=P(("grp", "sp"), "tp"),
        check_vma=False,
    )
```

```python
import functools

import jax
import jax.numpy as jnp
from jax import lax
from jax.experimental import pallas as pl
from jax.experimental.pallas import tpu as pltpu
from jax.sharding import PartitionSpec as P

H = 8
KVH = 2
HD = 128
WINDOW = 128
CONV = 3
EDGE = 16
MESH = pl.DeviceIdType.MESH
F32 = jnp.float32
BF16 = jnp.bfloat16


def layer_kernel(
    span,
    ranks,
    q_hbm,
    k_hbm,
    v_hbm,
    sink_ref,
    res_hbm,
    op_hbm,
    gain_hbm,
    wg_hbm,
    wu_hbm,
    cw_hbm,
    cb_hbm,
    wd_hbm,
    out_ref,
    gain_ref,
    cw_ref,
    cb_ref,
    q_buf,
    kv_buf,
    res_buf,
    op_buf,
    mix_buf,
    summed,
    stat,
    nx_buf,
    wide,
    tall,
    accs,
    act_buf,
    theirs_out,
    theirs_in,
    hop_out,
    hop_in,
    held,
    out_buf,
    out_sem,
    load_sem,
    kv_send,
    kv_recv,
    z_send,
    z_recv,
    y_send,
    y_recv,
    x_send,
    x_recv,
    edge_send,
    edge_recv,
    pair_send,
    pair_recv,
    hop_send,
    hop_recv,
):
    tokens, width = res_buf.shape
    depth, hidden = wg_hbm.shape
    cols = width // ranks
    quad_of = cols // depth
    half = span // 2
    pw = wide.shape[2]
    pd = tall.shape[2]
    chips = ranks // 2

    g = lax.axis_index("grp")
    s = lax.axis_index("sp")
    t = lax.axis_index("tp")
    right, left = lax.rem(s + 1, span), lax.rem(s + span - 1, span)
    parity = lax.rem(g, 2)
    pair_grp = g + 1 - 2 * parity
    own, other = 2 * parity, 2 - 2 * parity
    core = lax.rem(t, 2)
    chip = lax.div(t, 2)
    partner = t + 1 - 2 * core
    ahead = lax.rem(t + 2 - 4 * core + ranks, ranks)
    behind = lax.rem(t - 2 + 4 * core + ranks, ranks)
    across = lax.rem(t + ranks // 2, ranks)
    kv_col = pl.multiple_of(lax.div(t * KVH, ranks) * HD, HD)

    def rows(j):
        return pl.ds(pl.multiple_of(j * depth, depth), depth)

    own_rows = rows(s)
    cut = pw - (hidden - pw)
    def own_copies(sem, pairs):
        return [pltpu.make_async_copy(src, dst, load_sem.at[sem]) for src, dst in pairs]

    def loaded(sem, ref):
        pltpu.make_async_copy(ref, ref, load_sem.at[sem]).wait()

    rest = hidden - pw
    loads = own_copies(
        0,
        [
            (wg_hbm.at[:, pl.ds(0, pw)], wide.at[0, own_rows, :]),
            (wg_hbm.at[:, pl.ds(pw, rest)], wide.at[1, own_rows, pl.ds(0, rest)]),
            (wu_hbm.at[:, pl.ds(0, cut)], wide.at[1, own_rows, pl.ds(rest, cut)]),
            (wu_hbm.at[:, pl.ds(cut, pw)], wide.at[2, own_rows, :]),
        ],
    )
    loads += own_copies(1, [(wd_hbm.at[:, pl.ds(p * pd, pd)], tall.at[p, own_rows, :]) for p in range(3)])
    loads += own_copies(
        2,
        [
            (k_hbm.at[:, pl.ds(kv_col, HD)], kv_buf.at[0, pl.ds(WINDOW, tokens), :]),
            (v_hbm.at[:, pl.ds(kv_col, HD)], kv_buf.at[1, pl.ds(WINDOW, tokens), :]),
        ],
    )
    small = [(q_hbm, q_buf), (op_hbm, op_buf.at[t]), (res_hbm, res_buf), (gain_hbm, gain_ref), (cw_hbm, cw_ref), (cb_hbm, cb_ref)]
    single = [own_copies(3 + i, [pair])[0] for i, pair in enumerate(small)]
    loads += single

    barrier = pltpu.get_barrier_semaphore()
    greeted = ({"sp": right}, {"sp": left}, {"grp": pair_grp}, {"tp": ahead}, {"tp": behind}, {"tp": partner})
    for who in greeted:
        pl.semaphore_signal(barrier, inc=1, device_id=who, device_id_type=MESH)
    for copy in loads:
        copy.start()

    def remote(src, dst, send, recv, who):
        return pltpu.make_async_remote_copy(
            src_ref=src, dst_ref=dst, send_sem=send, recv_sem=recv, device_id=who, device_id_type=MESH
        )

    def part(kind, index, j):
        return (wide if kind == 0 else tall).at[index, rows(j), :]

    def z_copy(kind, ab, j, way, turns):
        ref = part(kind, own if ab else 1, j)
        row = 2 * kind + ab
        recv = z_recv.at[way, row, lax.rem(turns, 4)]
        return remote(ref, ref, z_send.at[way, row], recv, {"sp": left if way else right})

    def y_copy(kind, j):
        ref = part(kind, own, j)
        return remote(ref, ref, y_send.at[kind], y_recv.at[kind, lax.div(j, quad_of)], {"grp": pair_grp})

    def y_arrived(kind, quad):
        def wait(n):
            buf = wide if kind == 0 else tall
            ref = buf.at[other, pl.ds(pl.multiple_of(quad * cols, cols), n * depth), :]
            remote(ref, ref, y_send.at[kind], y_recv.at[kind, quad], {"grp": pair_grp}).wait_recv()

        is_own = quad == lax.div(s, quad_of)

        @pl.when(is_own)
        def _():
            wait(quad_of - 1)

        @pl.when(jnp.logical_not(is_own))
        def _():
            wait(quad_of)

    def block(kind, b):
        if kind == 0:
            return op_buf.at[b]
        return mix_buf.at[:, pl.ds(pl.multiple_of(b * HD, HD), HD)]

    def x_copy(kind, b, slot, who):
        ref = block(kind, b)
        return remote(ref, ref, x_send.at[kind], x_recv.at[kind, b], {"tp": who})

    def x_open(kind):
        x_copy(kind, t, 0, ahead).start()
        x_copy(kind, t, 1, behind).start()
        x_copy(kind, t, 2, partner).start()

    def x_pass(kind):
        x_copy(kind, behind, 3, ahead).wait_recv()
        x_copy(kind, behind, 3, ahead).start()
        x_copy(kind, behind, 4, partner).start()
        x_copy(kind, ahead, 5, partner).wait_recv()
        x_copy(kind, ahead, 5, partner).start()

    def x_last(kind):
        x_copy(kind, across, 6, partner).wait_recv()
        x_copy(kind, across, 6, partner).start()

    def x_close(kind):
        for step in range(chips):
            b = lax.rem(partner + 2 * step, ranks)
            x_copy(kind, b, 0, partner).wait_recv()

    def kv_copy(way):
        here, there = (tokens, 0) if way == 0 else (WINDOW, WINDOW + tokens)
        src, dst = kv_buf.at[core, pl.ds(here, WINDOW), :], kv_buf.at[core, pl.ds(there, WINDOW), :]
        return remote(src, dst, kv_send, kv_recv.at[way, core], {"sp": left if way else right})

    def kv_hand(way, which):
        ref = kv_buf.at[which, pl.ds(WINDOW + tokens if way else 0, WINDOW), :]
        return remote(ref, ref, kv_send, kv_recv.at[way, which], {"tp": partner})

    side = width // 2

    def edge_copy(way):
        here, there = (tokens, 0) if way == 0 else (EDGE, EDGE + tokens)
        lanes = pl.ds(pl.multiple_of(core * side, side), side)
        src, dst = nx_buf.at[pl.ds(here, EDGE), lanes], nx_buf.at[pl.ds(there, EDGE), lanes]
        return remote(src, dst, edge_send, edge_recv.at[way, core], {"sp": left if way else right})

    def edge_hand(way, which):
        lanes = pl.ds(pl.multiple_of(which * side, side), side)
        ref = nx_buf.at[pl.ds(EDGE + tokens if way else 0, EDGE), lanes]
        return remote(ref, ref, edge_send, edge_recv.at[way, which], {"tp": partner})

    def attend(i):
        lo = i * WINDOW
        keys = kv_buf[0, lo : lo + 3 * WINDOW, :]
        vals = kv_buf[1, lo : lo + 3 * WINDOW, :]
        scores = lax.dot_general(
            q_buf[lo : lo + WINDOW, :], keys, (((1,), (1,)), ((), ())), preferred_element_type=F32
        ) * (HD ** (-0.5))
        row = lax.broadcasted_iota(jnp.int32, scores.shape, 0)
        col = lax.broadcasted_iota(jnp.int32, scores.shape, 1)
        pos = s * tokens + (lo - WINDOW) + col
        gap = col - row
        seen = (gap >= 0) & (gap <= 2 * WINDOW) & (pos >= 0) & (pos < span * tokens)
        scores = jnp.where(seen, scores, F32(-1e30))
        sink = sink_ref[0]
        top = jnp.maximum(jnp.max(scores, axis=-1, keepdims=True), sink)
        expo = jnp.exp(scores - top)
        total = jnp.sum(expo, axis=-1, keepdims=True) + jnp.exp(sink - top)
        weights = (expo / total).astype(BF16)
        mixed = jnp.dot(weights, vals, preferred_element_type=F32).astype(BF16)
        mix_buf[lo : lo + WINDOW, pl.ds(pl.multiple_of(t * HD, HD), HD)] = mixed

    def project(o, opens):
        at = pl.ds(pl.multiple_of(o * cols, cols), cols)
        block_sum = res_buf[:, at].astype(F32) + jnp.dot(mix_buf[...], op_buf[o], preferred_element_type=F32)
        summed[:, at] = block_sum
        first, second = block_sum[:, : cols // 2], block_sum[:, cols // 2 :]
        lone = first + second
        squares = first * first + second * second
        if opens:
            stat[0] = lone
            stat[1] = squares
        else:
            stat[0] += lone
            stat[1] += squares

    def normalize(lo, hi):
        @pl.loop(lo // EDGE, hi // EDGE)
        def _(i):
            at = pl.ds(pl.multiple_of(i * EDGE, EDGE), EDGE)
            mean = jnp.sum(stat[0, at, :], axis=-1, keepdims=True) / width
            msq = jnp.sum(stat[1, at, :], axis=-1, keepdims=True) / width
            scale = lax.rsqrt(msq - mean * mean + 1e-05)
            normed = (summed[at, :] - mean) * scale * gain_ref[...]
            nx_buf[pl.ds(pl.multiple_of(i * EDGE + EDGE, EDGE), EDGE), :] = normed.astype(BF16)

    mid = tokens // 2
    lots = [slice(0, mid), slice(mid, tokens)]
    parcels = [slice(q * tokens // 4, (q + 1) * tokens // 4) for q in range(4)]
    quads = span * depth // cols
    mine = lax.div(s * depth, cols)

    def gates(shift, first=False):
        quad = lax.rem(mine + shift + quads, quads)
        at = pl.ds(pl.multiple_of(quad * cols, cols), cols)

        def add(p):
            y = jnp.dot(nx_buf[:, at], wide[p, at, :], preferred_element_type=F32)
            if first:
                accs[p] = y
            else:
                accs[p] += y

        add(1)
        add(own)
        y_arrived(0, quad)
        add(other)

    def edge_zero(where):
        for p in range(2):
            accs[p, where : where + EDGE, :] = jnp.zeros((EDGE, pw), F32)

    def activate(half_of):
        for h in range(3):
            gp, gc = divmod(h * pd, pw)
            up, uc = divmod(hidden + h * pd, pw)
            for r in range(half_of * mid, (half_of + 1) * mid, WINDOW):
                conv = cb_ref[h * pd : (h + 1) * pd].reshape(1, pd)
                for tap in range(CONV):
                    lo = EDGE - CONV // 2 + tap + r
                    gate = accs[gp, lo : lo + WINDOW, gc : gc + pd].astype(BF16).astype(F32)
                    conv = conv + gate * cw_ref[tap : tap + 1, h * pd : (h + 1) * pd]
                ups = accs[up, EDGE + r : EDGE + r + WINDOW, uc : uc + pd].astype(BF16).astype(F32)
                act = conv / (1.0 + jnp.exp(-conv)) * ups
                act_buf[r : r + WINDOW, h * pd : (h + 1) * pd] = act.astype(BF16)

    def partial(o, h):
        lot = lots[h]
        if h == 0:
            y_arrived(1, o)

        at = pl.ds(pl.multiple_of(o * cols, cols), cols)
        total = None
        for p in range(3):
            term = lax.dot_general(
                act_buf[lot, p * pd : (p + 1) * pd],
                tall[p, at, :],
                (((1,), (1,)), ((), ())),
                preferred_element_type=F32,
            )
            total = term if total is None else total + term
        return total

    def pair_copy(owner, h):
        src, dst = theirs_out.at[owner, lots[h]], theirs_in.at[owner, lots[h]]
        return remote(src, dst, pair_send, pair_recv.at[owner, h], {"tp": partner})

    def hop_copy(i, q):
        src, dst = hop_out.at[i, parcels[q]], hop_in.at[i, parcels[q]]
        return remote(src, dst, hop_send, hop_recv.at[i, q], {"tp": behind if i == 1 else ahead})

    def out_copy(q):
        return pltpu.make_async_copy(out_buf.at[parcels[q], :], out_ref.at[parcels[q], :], out_sem)

    def give(owner, h):
        theirs_out[owner, lots[h]] = partial(2 * owner + 1 - core, h).astype(BF16)
        pair_copy(owner, h).start()

    def joined(owner, h):
        kept = partial(2 * owner + core, h)
        pair_copy(owner, h).wait_recv()
        return kept + theirs_in[owner, lots[h]].astype(F32)

    def hop(i, owner, h):
        hop_out[i, lots[h]] = joined(owner, h).astype(BF16)
        hop_copy(i, 2 * h).start()
        hop_copy(i, 2 * h + 1).start()

    blocks = tokens // WINDOW

    def attend_inner():
        for i in range(1, blocks - 1):
            attend(i)

    def unit_attend(inner):
        if inner:
            for way in range(2):
                kv_copy(way).wait_recv()
                kv_hand(way, core).start()
            pl.when(core == 0)(attend_inner)
        else:
            for way in range(2):
                kv_hand(way, 1 - core).wait_recv()
            attend(0)
            attend(blocks - 1)
            x_open(1)

    def unit_edge():
        for way in range(2):
            edge_copy(way).wait_recv()
            edge_hand(way, core).start()

    def mirror(b):
        return b + 1 - 2 * lax.rem(b, 2)

    def unit_project(stage):
        if stage == 0:
            x_close(1)
            for copy in single[2:]:
                copy.wait()
            project(t, True)
            project(ahead, False)
        if stage == 1:
            x_last(0)
            x_copy(0, partner, 0, partner).wait_recv()
            project(behind, False)
            project(partner, False)
        if stage == 2:
            for b in (mirror(ahead), mirror(behind)):
                x_copy(0, b, 0, partner).wait_recv()
                project(b, False)
        if stage == 3:
            x_copy(0, mirror(across), 0, partner).wait_recv()
            project(across, False)
            project(mirror(across), False)

    quarter = tokens // 4

    def unit_normalize(i, send=False):
        normalize(i * quarter, (i + 1) * quarter)
        if send:
            for way in range(2):
                edge_copy(way).start()

    def unit_gates(shifts, first=False):
        if first:
            for way in range(2):
                edge_hand(way, 1 - core).wait_recv()
        for i, shift in enumerate(shifts):
            gates(shift, first and i == 0)

    loaded(0, wide.at[:, own_rows, :])
    loaded(1, tall.at[:, own_rows, :])
    loaded(2, kv_buf.at[:, pl.ds(WINDOW, tokens), :])
    single[0].wait()
    pl.semaphore_wait(barrier, len(greeted))

    @pl.when(core == 1)
    def _():
        attend_inner()

    for kind in range(2):
        for turn in range(2):
            for way in range(2):
                z_copy(kind, turn if way == 0 else 1 - turn, s, way, 1).start()
        if kind == 0:
            for way in range(2):
                kv_copy(way).start()
    single[1].wait()
    x_open(0)

    units = {
        (1, 0): lambda: unit_attend(True),
        (1, 1): lambda: unit_attend(False),
        (3, 0): lambda: x_pass(0),
        (3, 1): lambda: x_pass(1),
        (6, 0): lambda: x_last(1),
        (6, 1): lambda: unit_project(0),
        (7, 0): lambda: unit_project(1),
        (7, 1): lambda: unit_project(2),
        (8, 0): lambda: unit_project(3),
        (8, 1): lambda: unit_normalize(0),
        (9, 0): lambda: unit_normalize(3, True),
        (9, 1): lambda: unit_normalize(1),
        (10, 0): lambda: unit_normalize(2),
        (10, 1): unit_edge,
        (11, 1): lambda: unit_gates([0], True),
        (12, 0): lambda: unit_gates([1]),
        (12, 1): lambda: unit_gates([-1]),
        (13, 0): lambda: unit_gates([2]),
        (13, 1): lambda: unit_gates([-2]),
    }

    def hop_on(kind, k, swap, turns=(0, 1)):
        back = lax.rem(s - k + span, span)
        front = lax.rem(s + k, span)
        for turn in turns:
            for way, j in ((0, back), (1, front)):
                ab = turn if way == 0 else 1 - turn
                z_copy(kind, ab, j, way, k).wait_recv()
                if ab == way:
                    z_copy(kind, ab, j, way, k + 1).start()
                else:

                    @pl.when(k < half - 1)
                    def _():
                        z_copy(kind, ab, j, way, k + 1).start()

                if ab == 1 and swap is not False:
                    pl.when(swap)(y_copy(kind, j).start)

    def swap_down(k):
        y_copy(1, lax.rem(s - k + span, span)).start()
        y_copy(1, lax.rem(s + k, span)).start()

    def ring_wide(k):
        hop_on(0, k, True)

    def ring_tall(k):
        hop_on(1, k, k < half - 1)

    @pl.loop(1, half)
    def _(k):
        ring_wide(k)
        for (step, slot), unit in units.items():
            if slot == 0:
                pl.when(k == step)(unit)

        ring_tall(k)
        for (step, slot), unit in units.items():
            if slot == 1:
                pl.when(k == step)(unit)

    far = lax.rem(s + half, span)
    z_copy(0, 1, far, 1, half).wait_recv()
    y_copy(0, far).start()
    swap_down(half - 1)
    z_copy(0, 0, far, 0, half).wait_recv()

    gates(3)
    gates(-3)
    z_copy(1, 1, far, 1, half).wait_recv()
    y_copy(1, far).start()
    gates(4)

    @pl.when(s == 0)
    def _():
        edge_zero(0)

    @pl.when(s == span - 1)
    def _():
        edge_zero(EDGE + tokens)

    chip_across = lax.div(across, 2)
    chip_ahead = lax.div(ahead, 2)
    chip_behind = lax.div(behind, 2)
    own_cols = pl.ds(pl.multiple_of(t * cols, cols), cols)

    activate(0)
    z_copy(1, 0, far, 0, half).wait_recv()
    give(chip_across, 0)
    activate(1)
    give(chip_across, 1)
    hop(0, chip_across, 0)
    give(chip_ahead, 0)
    hop(0, chip_across, 1)
    give(chip_ahead, 1)
    hop(1, chip_behind, 0)
    give(chip_behind, 0)
    hop(1, chip_behind, 1)
    give(chip_behind, 1)
    held[0, lots[0]] = joined(chip_ahead, 0)
    give(chip, 0)
    held[0, lots[1]] = joined(chip_ahead, 1)
    give(chip, 1)
    for h in range(2):
        for q in (2 * h, 2 * h + 1):
            hop_copy(0, q).wait_recv()
            hop_out[2, parcels[q]] = (held[0, parcels[q]] + hop_in[0, parcels[q]].astype(F32)).astype(BF16)
            hop_copy(2, q).start()
        own_normed = nx_buf[EDGE + h * mid : EDGE + (h + 1) * mid, own_cols].astype(F32)
        held[1, lots[h]] = joined(chip, h) + own_normed
    for q in range(4):
        hop_copy(1, q).wait_recv()
        hop_copy(2, q).wait_recv()
        terms = hop_in[1, parcels[q]].astype(F32) + hop_in[2, parcels[q]].astype(F32)
        out_buf[parcels[q], :] = (held[1, parcels[q]] + terms).astype(BF16)
        out_copy(q).start()

    pltpu.make_async_copy(out_buf, out_ref, out_sem).wait()

    def left_all(ref, send, recv):
        remote(ref, ref, send, recv, {"tp": partner}).wait_send()

    left_all(kv_buf.at[0, pl.ds(0, 4 * WINDOW), :], kv_send, kv_recv.at[0, 0])
    left_all(nx_buf.at[pl.ds(0, 2 * EDGE), :], edge_send, edge_recv.at[0, 0])
    left_all(theirs_out, pair_send, pair_recv.at[0, 0])
    left_all(hop_out, hop_send, hop_recv.at[0, 0])
    for way in range(2):
        for kind in range(2):
            for ab in range(2):
                n = half if ab == way else half - 1
                ref = (wide if kind == 0 else tall).at[0, pl.ds(0, n * depth), :]
                row = 2 * kind + ab
                remote(ref, ref, z_send.at[way, row], z_recv.at[way, row, 0], {"sp": right}).wait_send()
    for kind in range(2):
        ref = (wide if kind == 0 else tall).at[0, pl.ds(0, (span - 1) * depth), :]
        remote(ref, ref, y_send.at[kind], y_recv.at[kind, 0], {"grp": pair_grp}).wait_send()
        ref = op_buf.at[pl.ds(0, ranks - 1)] if kind == 0 else mix_buf.at[:, pl.ds(0, (ranks - 1) * HD)]
        remote(ref, ref, x_send.at[kind], x_recv.at[kind, 0], {"tp": partner}).wait_send()


def solution(mesh):
    span, ranks = mesh.shape["sp"], mesh.shape["tp"]

    def shards(q, k, v, sink, resid, out_proj, gain, w_gate, w_up, conv_w, conv_b, w_down):
        tokens, width = resid.shape
        depth, hidden = w_gate.shape
        cols = width // ranks
        chips = ranks // 2
        pw, pd = 2 * hidden // 3, hidden // 3
        there = pl.BlockSpec(memory_space=pltpu.HBM)
        scalar = pl.BlockSpec(memory_space=pltpu.SMEM)
        dma = pltpu.SemaphoreType.DMA
        return pl.pallas_call(
            functools.partial(layer_kernel, span, ranks),
            out_shape=jax.ShapeDtypeStruct((tokens, cols), BF16),
            in_specs=[there, there, there, scalar] + [there] * 8,
            out_specs=there,
            scratch_shapes=[
                pltpu.VMEM((1, width), F32),
                pltpu.VMEM(conv_w.shape, F32),
                pltpu.VMEM(conv_b.shape, F32),
                pltpu.VMEM((tokens, HD), BF16),
                pltpu.VMEM((2, tokens + 2 * WINDOW, HD), BF16),
                pltpu.VMEM((tokens, width), BF16),
                pltpu.VMEM((ranks, out_proj.shape[0], cols), BF16),
                pltpu.VMEM((tokens, ranks * HD), BF16),
                pltpu.VMEM((tokens, width), F32),
                pltpu.VMEM((2, tokens, cols // 2), F32),
                pltpu.VMEM((tokens + 2 * EDGE, width), BF16),
                pltpu.VMEM((3, span * depth, pw), BF16),
                pltpu.VMEM((3, span * depth, pd), BF16),
                pltpu.VMEM((3, tokens + 2 * EDGE, pw), F32),
                pltpu.VMEM((tokens, hidden), BF16),
                pltpu.VMEM((chips, tokens, cols), BF16),
                pltpu.VMEM((chips, tokens, cols), BF16),
                pltpu.VMEM((3, tokens, cols), BF16),
                pltpu.VMEM((3, tokens, cols), BF16),
                pltpu.VMEM((2, tokens, cols), F32),
                pltpu.VMEM((tokens, cols), BF16),
                dma(()),
                dma((9,)),
                dma(()),
                dma((2, 2)),
                dma((2, 4)),
                dma((2, 4, 4)),
                dma((2,)),
                dma((2, ranks)),
                dma((2,)),
                dma((2, ranks)),
                dma(()),
                dma((2, 2)),
                dma(()),
                dma((chips, 2)),
                dma(()),
                dma((3, 4)),
            ],
            compiler_params=pltpu.CompilerParams(
                collective_id=0, has_side_effects=True, vmem_limit_bytes=60 * 1024 * 1024
            ),
        )(
            q, k, v, sink, resid, out_proj, gain.reshape(1, width), w_gate, w_up,
            conv_w, conv_b, w_down.T,
        )

    return jax.shard_map(
        shards,
        mesh=mesh,
        in_specs=(
            P(("grp", "sp"), "tp"),
            P(("grp", "sp"), None),
            P(("grp", "sp"), None),
            P("tp"),
            P(("grp", "sp"), None),
            P(None, "tp"),
            P(),
            P("sp", "tp"),
            P("sp", "tp"),
            P(None, "tp"),
            P("tp"),
            P("tp", "sp"),
        ),
        out_specs=P(("grp", "sp"), "tp"),
        check_vma=False,
    )
```
